256 devices in a mesh: grp: 2 (over y), st: 32 (over z, core), tp: 4 (over x).
Axes of the slice: x: 4, y: 2, z: 16, core: 2. Of those that a mesh axis runs over, the one named last changes fastest.
The devices are a block of a 4x16x16 slice.
Arguments:
- tokens: bfloat16 [32768, 2048], P(('grp', 'st'), 'tp'), parts along dimension 0, may hold values from -180 to 180
- ret_query: bfloat16 [32768, 1024], P(('grp', 'st'), 'tp'), parts along dimension 0, may hold values from -6 to 6
- ret_key: bfloat16 [32768, 1024], P(('grp', 'st'), 'tp'), parts along dimension 0, may hold values from -6 to 6
- ret_value: bfloat16 [32768, 1024], P(('grp', 'st'), 'tp'), parts along dimension 0, may hold values from -6 to 6
- w_query: bfloat16 [2048, 2048], P(None, 'tp'), may hold values from -0.125 to 0.125
- w_key: bfloat16 [2048, 2048], P(None, 'tp'), may hold values from -0.125 to 0.125
- w_value: bfloat16 [2048, 2048], P(None, 'tp'), may hold values from -0.125 to 0.125
- w_gate: bfloat16 [2048, 4], replicated, may hold values from -0.125 to 0.125
- store: bfloat16 [192, 128, 2048], P('st'), may hold values from -6 to 6
- passage_ids: int32 [512, 4], P(('grp', 'st')), parts along dimension 0, may hold values from 0 to 191, as said below
Outputs:
- blended: bfloat16 [32768, 3072], P(('grp', 'st'), 'tp'), parts along dimension 0
The draws below stay inside these ranges and needn't reach their ends.
There are 2 independent parts, one for each index of `grp`. The reference program is written for one: setup_inputs(seed, part) draws one part's arguments, and reference() takes and returns one part's arrays. A program takes and returns all parts, laid end to end along the dimension named above; an argument that names none is the same for every part. Nothing has to cross between parts.
Inputs may be any that keep to these rules, and one draw needn't show every extreme that they name: `passage_ids`: passage p lies on index p // 6 of st. The 8 rows of one device name passages of any one index of st at most 2 times in all, and those of some index exactly 2 times.
All inputs are finite; a program needn't handle non-finite values.
Results may differ from the reference program's by a relative error of at most 0.0094.
Values may be sent and summed in bfloat16 or wider, within the bound.
A program may use at most 128 MiB of HBM per device.

```python
import jax
import jax.numpy as jnp
from jax import lax

D = 2048
HEADS = 4
RET_DIM = 256
HEAD_DIM = 512
PROWS = 128
BLOCK = 64
NPB = 4
TOK_DEV = 512
PASS_DEV = 6
SEQ_LEN = 256
TOKENS = 16384
BLK_DEV = 8
NBLK = 256
PASSAGES = 192
CAP = 2
N_ST = 32


def draw_tokens(key, part):
    layout = (TOK_DEV * N_ST, D)
    values = 1.5 * jax.random.truncated_normal(jax.random.fold_in(key, 11), -6.0, 6.0, layout, jnp.float32)
    return values.astype(jnp.bfloat16)


def requests_for(subkey, device):
    entries = jnp.arange(N_ST * CAP, dtype=jnp.int32)
    owner_of = entries // CAP
    copy_of = entries % CAP
    full_owner = (device + jax.random.randint(jax.random.fold_in(subkey, 1), (), 0, N_ST // 2)) % N_ST
    before_owner = (device + N_ST - 1) % N_ST
    across_owner = (device + N_ST // 2) % N_ST
    forced = (owner_of == full_owner) | (copy_of == 0) & ((owner_of == before_owner) | (owner_of == across_owner))
    popular = jax.random.randint(jax.random.fold_in(subkey, 2), (N_ST,), 0, 131072)
    jitter = jax.random.randint(jax.random.fold_in(subkey, 3), (N_ST * CAP,), 0, 32768)
    priority = jnp.where(forced, 524288, jnp.take(popular, owner_of) + jitter) * 1024 + entries
    _, chosen = lax.top_k(priority, BLK_DEV * NPB)
    within = jax.random.randint(jax.random.fold_in(subkey, 4), (BLK_DEV * NPB,), 0, PASS_DEV)
    picked = jnp.take(owner_of, chosen) * PASS_DEV + within
    return jax.random.permutation(jax.random.fold_in(subkey, 5), picked)


def draw_passage_ids(key, part):
    subkeys = jax.random.split(jax.random.fold_in(key, 21), N_ST)
    picked = jax.vmap(requests_for)(subkeys, jnp.arange(N_ST, dtype=jnp.int32))
    return picked.reshape(N_ST * BLK_DEV, NPB).astype(jnp.int32)


def level_of(rng, dims, cuts, least, high):
    def one(position, parts):
        steps = jax.random.uniform(jax.random.fold_in(jax.random.fold_in(rng, 6), position), (parts,), jnp.float32, least / len(cuts), high / len(cuts))
        return jnp.repeat(jnp.exp(steps), dims[position] // parts).reshape((-1,) + (1,) * (len(dims) - position - 1))

    gain = one(*cuts[0])
    for cut in cuts[1:]:
        gain = gain * one(*cut)
    return gain


def gaussian(own_key, extent, width, limit, shards=(), kind=jnp.bfloat16):
    gain = level_of(own_key, extent, shards, -0.22, 0.18) if shards else 1.0
    values = jax.random.normal(own_key, extent, jnp.float32) * width * gain
    return jnp.minimum(jnp.maximum(values, -limit), limit).astype(kind)


def setup_inputs(seed: int = 0, part: int = 0) -> dict:
    seeds = jax.random.split(jax.random.key(seed), 11)
    part_keys = jax.random.split(jax.random.fold_in(seeds[10], part), 11)
    return {
        "tokens": draw_tokens(jax.random.fold_in(jax.random.fold_in(seeds[10], part), 71), part),
        "ret_query": gaussian(part_keys[1], (TOKENS, HEADS * RET_DIM), 1.0, 6.0, ((0, 32), (1, 4))),
        "ret_key": gaussian(part_keys[2], (TOKENS, HEADS * RET_DIM), 1.0, 6.0, ((0, 32), (1, 4))),
        "ret_value": gaussian(part_keys[3], (TOKENS, HEADS * RET_DIM), 1.0, 6.0, ((0, 32), (1, 4))),
        "w_query": gaussian(seeds[4], (D, HEADS * HEAD_DIM), D ** -0.5, 0.125, ((1, 4),)),
        "w_key": gaussian(seeds[5], (D, HEADS * HEAD_DIM), D ** -0.5, 0.125, ((1, 4),)),
        "w_value": gaussian(seeds[6], (D, HEADS * HEAD_DIM), D ** -0.5, 0.125, ((1, 4),)),
        "w_gate": gaussian(seeds[7], (D, HEADS), D ** -0.5, 0.125),
        "store": gaussian(seeds[8], (PASSAGES, PROWS, D), 1.0, 6.0, ((0, 32),)),
        "passage_ids": draw_passage_ids(jax.random.fold_in(jax.random.fold_in(seeds[10], part), 71), part),
    }


ROTARY_BASE = 10000.0
NORM_EPS = 1e-05

def rounded(values):
    return lax.optimization_barrier(values.astype(jnp.bfloat16)).astype(jnp.float32)

def rotate(values, positions):
    halfway = values.shape[-1] // 2
    inverse = ROTARY_BASE ** (-jnp.arange(halfway, dtype=jnp.float32) / halfway)
    angles = positions.astype(jnp.float32)[:, None, None] * inverse
    cosines, sines = (jnp.cos(angles), jnp.sin(angles))
    leading, trailing = (values[..., :halfway], values[..., halfway:])
    return jnp.concatenate([leading * cosines - trailing * sines, leading * sines + trailing * cosines], axis=-1)

def retain_all(query_rows, key_rows, value_rows):
    layout = (TOKENS // SEQ_LEN, SEQ_LEN, HEADS, RET_DIM)
    places = jnp.arange(SEQ_LEN, dtype=jnp.int32)
    rot_query = rounded(rotate(query_rows.reshape(layout).astype(jnp.float32), places))
    rot_key = rounded(rotate(key_rows.reshape(layout).astype(jnp.float32), places) * RET_DIM ** (-0.5))
    head_number = jnp.arange(HEADS, dtype=jnp.float32)
    log_gamma = jnp.log1p(-jnp.exp2(-5.0 - head_number))
    offsets = (places[:, None] - places[None, :]).astype(jnp.float32)
    decays = jnp.where(offsets[None] >= 0.0, jnp.exp(log_gamma[:, None, None] * jnp.maximum(offsets, 0.0)[None]), 0.0)
    scores = jnp.einsum('sigd,sjgd->sgij', rot_query, rot_key)
    weights = rounded(scores * decays[None])
    output = jnp.einsum('sgij,sjge->sige', weights, value_rows.reshape(layout).astype(jnp.float32))
    centred = output - lax.optimization_barrier(jnp.mean(output, -1, keepdims=True))
    normed = centred * lax.rsqrt(lax.optimization_barrier(jnp.mean(centred * centred, -1, keepdims=True)) + NORM_EPS)
    return normed.astype(jnp.bfloat16).reshape(TOKENS, HEADS, RET_DIM)

def reference(tokens, ret_query, ret_key, ret_value, w_query, w_key, w_value, w_gate, store, passage_ids):
    retained = retain_all(ret_query, ret_key, ret_value)
    queries = jnp.dot(tokens, w_query, preferred_element_type=jnp.float32).astype(jnp.bfloat16)
    gate_vals = jax.nn.sigmoid(jnp.dot(tokens, w_gate, preferred_element_type=jnp.float32))
    keys_all = jnp.dot(store, w_key, preferred_element_type=jnp.float32).astype(jnp.bfloat16)
    values_all = jnp.dot(store, w_value, preferred_element_type=jnp.float32).astype(jnp.bfloat16)

    def attend(inputs):
        query_block, id_row, gate_block = inputs
        key_sel = jnp.take(keys_all, id_row, axis=0).reshape(NPB, PROWS, HEADS, HEAD_DIM).astype(jnp.float32)
        value_sel = jnp.take(values_all, id_row, axis=0).reshape(NPB, PROWS, HEADS, HEAD_DIM).astype(jnp.float32)
        scores = jnp.einsum('thd,jrhd->jhtr', query_block.astype(jnp.float32), key_sel) * HEAD_DIM ** (-0.5)
        highest = lax.optimization_barrier(jnp.max(scores, -1))
        exponent = jnp.exp(scores - highest[..., None])
        totals = lax.optimization_barrier(jnp.sum(exponent, -1))
        weighted = rounded(jnp.einsum('jhtr,jrhd->jthd', rounded(exponent), value_sel))
        overall = lax.optimization_barrier(jnp.max(highest, 0))
        scales = jnp.exp(highest - overall[None])
        denominator = lax.optimization_barrier(jnp.sum(scales * totals, 0))
        numerator = lax.optimization_barrier(jnp.sum(jnp.transpose(scales, (0, 2, 1))[..., None] * weighted, 0))
        return (gate_block[..., None] * numerator / jnp.transpose(denominator)[..., None]).astype(jnp.bfloat16)
    retrieved = lax.map(attend, (queries.reshape(NBLK, BLOCK, HEADS, HEAD_DIM), passage_ids, gate_vals.reshape(NBLK, BLOCK, HEADS)))
    retrieved = retrieved.reshape(TOKENS, HEADS, HEAD_DIM)
    return jnp.concatenate([retained, retrieved], -1).reshape(TOKENS, HEADS * (RET_DIM + HEAD_DIM))
```

```python
import functools

import jax
import jax.numpy as jnp
from jax import lax
from jax.experimental import pallas as pl
from jax.experimental.pallas import tpu as pltpu
from jax.sharding import PartitionSpec as P

RET_DIM = 256
HEAD_DIM = 512
BLOCK = 64
NPB = 4
SEQ_LEN = 256
CAP = 2
CORES = 2
CHUNK = 128
ROTARY_BASE = 10000.0
NORM_EPS = 1e-05
MASKED = -1e30
FLOOR = -1e28


def rotate(values, positions):
    halfway = values.shape[-1] // 2
    inverse = ROTARY_BASE ** (-jnp.arange(halfway, dtype=jnp.float32) / halfway)
    angles = positions.astype(jnp.float32)[:, None, None] * inverse
    cosines, sines = (jnp.cos(angles), jnp.sin(angles))
    leading, trailing = (values[..., :halfway], values[..., halfway:])
    return jnp.concatenate(
        [leading * cosines - trailing * sines, leading * sines + trailing * cosines], axis=-1
    )


def retain(query_rows, key_rows, value_rows, head_start):
    token_count = query_rows.shape[0]
    groups = query_rows.shape[1] // RET_DIM
    layout = (token_count // SEQ_LEN, SEQ_LEN, groups, RET_DIM)
    places = jnp.arange(SEQ_LEN, dtype=jnp.int32)
    rot_query = rotate(query_rows.reshape(layout).astype(jnp.float32), places).astype(jnp.bfloat16)
    rot_key = (
        rotate(key_rows.reshape(layout).astype(jnp.float32), places) * RET_DIM ** (-0.5)
    ).astype(jnp.bfloat16)
    head_number = (head_start + jnp.arange(groups, dtype=jnp.int32)).astype(jnp.float32)
    log_gamma = jnp.log1p(-jnp.exp2(-5.0 - head_number))
    offsets = (places[:, None] - places[None, :]).astype(jnp.float32)
    decays = jnp.where(
        offsets[None] >= 0.0,
        jnp.exp(log_gamma[:, None, None] * jnp.maximum(offsets, 0.0)[None]),
        0.0,
    )
    scores = jnp.einsum("sigd,sjgd->sgij", rot_query, rot_key, preferred_element_type=jnp.float32)
    weights = (scores * decays[None]).astype(jnp.bfloat16)
    output = jnp.einsum(
        "sgij,sjge->sige", weights, value_rows.reshape(layout), preferred_element_type=jnp.float32
    )
    centred = output - jnp.mean(output, -1, keepdims=True)
    normed = centred * lax.rsqrt(jnp.mean(centred * centred, -1, keepdims=True) + NORM_EPS)
    return normed.astype(jnp.bfloat16).reshape(token_count, groups, RET_DIM)


def ring_kernel(
    pid_ref, blk_ref, q_ref, k_ref, v_ref, out_ref, ml_ref,
    qbuf, kall, vall, loc, locml, loc0, loc0ml, rbuf, rml,
    local_sem, kv_send, kv_recv, q_send, q_recv, r_send, r_recv, s_send, s_recv,
):
    devices = lax.axis_size("st")
    ring = devices // CORES
    far = ring // 2
    chunks = q_ref.shape[0]
    half = chunks // 2
    slots = CAP * CORES
    mine = lax.axis_index("st")
    place, core = mine // CORES, mine % CORES
    right = lax.rem(mine + CORES, devices)
    left = lax.rem(mine + devices - CORES, devices)
    partner = mine + 1 - 2 * core
    toward = (right, left)
    far_set = (tuple(range(half)), tuple(range(half, chunks)))

    barrier = pltpu.get_barrier_semaphore()
    for device in (right, left, partner):
        pl.semaphore_signal(barrier, inc=1, device_id={"st": device})
    pl.semaphore_wait(barrier, 3)

    def q_copy(way, hop, j):
        source = q_ref.at[j] if isinstance(hop, int) and hop == 1 else qbuf.at[way, jnp.maximum(hop - 2, 0), j]
        return pltpu.make_async_remote_copy(
            src_ref=source,
            dst_ref=qbuf.at[way, hop - 1, j],
            send_sem=q_send.at[way, hop - 1, j],
            recv_sem=q_recv.at[way, hop - 1, j],
            device_id={"st": toward[way]},
        )

    for j in range(chunks):
        for way in range(2):
            q_copy(way, 1, j).start()

    kv_copies = []
    for i, (own, everyone) in enumerate(((k_ref, kall), (v_ref, vall))):
        kv_copies.append(
            pltpu.make_async_remote_copy(
                src_ref=own,
                dst_ref=everyone.at[core],
                send_sem=kv_send.at[i],
                recv_sem=kv_recv.at[i],
                device_id={"st": partner},
            )
        )
    local_copies = [
        pltpu.make_async_copy(own, everyone.at[core], local_sem.at[i])
        for i, (own, everyone) in enumerate(((k_ref, kall), (v_ref, vall)))
    ]
    for copy in kv_copies:
        copy.start()
    for copy in local_copies:
        copy.start()
    for copy in local_copies:
        copy.wait()
    for copy in kv_copies:
        copy.wait()

    passages = k_ref.shape[0]
    lanes = lax.broadcasted_iota(jnp.int32, (1, CHUNK), 1)

    def attend(query, source, j):
        base = source * slots
        keys, values, penalties = [], [], []
        for slot in range(slots):
            passage = pid_ref[base + slot]
            block = blk_ref[base + slot]
            keys.append(kall[passage // passages, passage % passages])
            values.append(vall[passage // passages, passage % passages])
            within = block - j * (CHUNK // BLOCK)
            penalties.append(jnp.where(lanes // BLOCK == within, 0.0, MASKED))
        scores = [
            jnp.dot(key, query, preferred_element_type=jnp.float32) * HEAD_DIM ** (-0.5) + penalty
            for key, penalty in zip(keys, penalties)
        ]
        highest = jnp.full((1, CHUNK), FLOOR, jnp.float32)
        for score in scores:
            highest = jnp.maximum(highest, jnp.max(score, 0, keepdims=True))
        exponents = [jnp.exp(score - highest) for score in scores]
        total = jnp.zeros((1, CHUNK), jnp.float32)
        for exponent in exponents:
            total = total + jnp.sum(exponent, 0, keepdims=True)
        weighted = jnp.dot(
            jnp.concatenate(values, 1),
            jnp.concatenate([e.astype(jnp.bfloat16) for e in exponents], 0),
            preferred_element_type=jnp.float32,
        )
        return weighted, highest, total

    def source_of(way, hop):
        return lax.rem(place + (ring - hop if way == 0 else hop), ring)

    def attend_hop(hop, ways_chunks):
        for way, j in ways_chunks:
            weighted, highest, total = attend(qbuf[way, hop - 1, j], source_of(way, hop), j)
            loc[way, hop - 1, j] = weighted.astype(jnp.bfloat16)
            locml[way, hop - 1, j, 0:1] = highest
            locml[way, hop - 1, j, 1:2] = total

    @pl.loop(0, chunks)
    def _(j):
        weighted, highest, total = attend(q_ref[j], place, j)
        loc0[j] = weighted.astype(jnp.bfloat16)
        loc0ml[j, 0:1] = highest
        loc0ml[j, 1:2] = total

    def arrive(hop, forward):
        for j in range(chunks):
            for way in range(2):
                q_copy(way, hop, j).wait_recv()
                if j in forward[way]:
                    q_copy(way, hop + 1, j).start()

    everything = (tuple(range(chunks)),) * 2

    @pl.loop(1, far - 1)
    def _(hop):
        arrive(hop, everything)

        @pl.loop(0, chunks)
        def _(j):
            attend_hop(hop, [(0, j), (1, j)])

    arrive(far - 1, far_set)

    @pl.loop(0, chunks)
    def _(j):
        attend_hop(far - 1, [(0, j), (1, j)])

    def r_copies(way, hop, j):
        data = pltpu.make_async_remote_copy(
            src_ref=loc.at[1 - way, hop - 1, j],
            dst_ref=rbuf.at[way, hop - 1, j],
            send_sem=r_send.at[way, hop - 1, j],
            recv_sem=r_recv.at[way, hop - 1, j],
            device_id={"st": toward[way]},
        )
        stats = pltpu.make_async_remote_copy(
            src_ref=locml.at[1 - way, hop - 1, j],
            dst_ref=rml.at[way, hop - 1, j],
            send_sem=s_send.at[way, hop - 1, j],
            recv_sem=s_recv.at[way, hop - 1, j],
            device_id={"st": toward[way]},
        )
        return data, stats

    def r_start(way, hop, j):
        for copy in r_copies(way, hop, j):
            copy.start()

    def merge(first, first_ml, second, second_ml):
        top = jnp.maximum(first_ml[0], second_ml[0])
        left_scale, right_scale = jnp.exp(first_ml[0] - top), jnp.exp(second_ml[0] - top)
        summed = first * left_scale + second * right_scale
        total = first_ml[1] * left_scale + second_ml[1] * right_scale
        return summed, (top, total)

    def r_merge(way, hop, j):
        for copy in r_copies(way, hop + 1, j):
            copy.wait_recv()
        summed, (top, total) = merge(
            rbuf[way, hop, j].astype(jnp.float32),
            (rml[way, hop, j, 0:1], rml[way, hop, j, 1:2]),
            loc[1 - way, hop - 1, j].astype(jnp.float32),
            (locml[1 - way, hop - 1, j, 0:1], locml[1 - way, hop - 1, j, 1:2]),
        )
        loc[1 - way, hop - 1, j] = summed.astype(jnp.bfloat16)
        locml[1 - way, hop - 1, j, 0:1] = top
        locml[1 - way, hop - 1, j, 1:2] = total

    for i in range(half):
        for way in range(2):
            q_copy(way, far, far_set[way][i]).wait_recv()
        attend_hop(far, [(way, far_set[way][i]) for way in range(2)])
    for i in range(half):
        for way in range(2):
            r_start(way, far, far_set[1 - way][i])

    for i in range(half):
        for way in range(2):
            r_start(way, far - 1, far_set[way][i])
    for i in range(half):
        for way in range(2):
            r_merge(way, far - 1, far_set[1 - way][i])
        for way in range(2):
            r_start(way, far - 1, far_set[1 - way][i])

    @pl.loop(1, far - 1)
    def _(step):
        hop = far - 1 - step
        for j in range(chunks):
            order = [(way, (far_set[way] + far_set[1 - way])[j]) for way in range(2)]
            for way, chunk in order:
                r_merge(way, hop, chunk)
            for way, chunk in order:
                r_start(way, hop, chunk)

    for i in range(chunks):
        for way in range(2):
            for copy in r_copies(way, 1, (far_set[way] + far_set[1 - way])[i]):
                copy.wait_recv()

    @pl.loop(0, chunks)
    def _(j):
        summed, both = loc0[j].astype(jnp.float32), (loc0ml[j, 0:1], loc0ml[j, 1:2])
        for way in range(2):
            summed, both = merge(
                summed, both, rbuf[way, 0, j].astype(jnp.float32), (rml[way, 0, j, 0:1], rml[way, 0, j, 1:2])
            )
        out_ref[j] = summed
        ml_ref[j, 0:1] = both[0]
        ml_ref[j, 1:2] = both[1]

    for j in range(chunks):
        for way in range(2):
            q_copy(way, 1, j).wait_send()

    @pl.loop(2, far)
    def _(hop):
        for j in range(chunks):
            for way in range(2):
                q_copy(way, hop, j).wait_send()

    @pl.loop(1, far)
    def _(hop):
        for j in range(chunks):
            for way in range(2):
                for copy in r_copies(way, hop, j):
                    copy.wait_send()

    for way in range(2):
        for j in far_set[way]:
            q_copy(way, far, j).wait_send()
        for j in far_set[1 - way]:
            for copy in r_copies(way, far, j):
                copy.wait_send()


def ring_attend(pids, blocks, queries, keys, values):
    ring = lax.axis_size("st") // CORES
    far = ring // 2
    chunks, width, _ = queries.shape
    passages, rows, _ = keys.shape
    buffer = (2, far, chunks, width, CHUNK)
    stats = (2, far, chunks, 2, CHUNK)
    flags = (2, far, chunks)
    dma = pltpu.SemaphoreType.DMA
    return pl.pallas_call(
        ring_kernel,
        out_shape=(
            jax.ShapeDtypeStruct((chunks, width, CHUNK), jnp.float32),
            jax.ShapeDtypeStruct((chunks, 2, CHUNK), jnp.float32),
        ),
        in_specs=[pl.BlockSpec(memory_space=pltpu.SMEM)] * 2
        + [pl.BlockSpec(memory_space=pltpu.VMEM)] * 3,
        out_specs=(pl.BlockSpec(memory_space=pltpu.VMEM),) * 2,
        scratch_shapes=[
            pltpu.VMEM(buffer, jnp.bfloat16),
            pltpu.VMEM((CORES, passages, rows, width), jnp.bfloat16),
            pltpu.VMEM((CORES, passages, width, rows), jnp.bfloat16),
            pltpu.VMEM(buffer, jnp.bfloat16),
            pltpu.VMEM(stats, jnp.float32),
            pltpu.VMEM(buffer[2:], jnp.bfloat16),
            pltpu.VMEM(stats[2:], jnp.float32),
            pltpu.VMEM(buffer, jnp.bfloat16),
            pltpu.VMEM(stats, jnp.float32),
            dma((2,)),
            dma((2,)),
            dma((2,)),
            dma(flags),
            dma(flags),
            dma(flags),
            dma(flags),
            dma(flags),
            dma(flags),
        ],
        compiler_params=pltpu.CompilerParams(
            collective_id=0, has_side_effects=True, vmem_limit_bytes=60 * 1024 * 1024
        ),
    )(pids, blocks, queries, keys, values)


def slot_tables(passage_ids, per_chip):
    ring = lax.axis_size("st") // CORES
    mine = lax.axis_index("st")
    place, core = mine // CORES, mine % CORES
    ids = lax.all_gather(passage_ids.reshape(1, -1), "st", axis=0, tiled=True)
    ids = ids.reshape(ring, CORES, -1)
    ids = jnp.where(core == 0, ids[:, 0], ids[:, 1])
    hit = (ids // per_chip == place).astype(jnp.int32)
    requests = ids.shape[1]
    order = jnp.arange(requests, dtype=jnp.int32)
    earlier = (order[:, None] > order[None, :]).astype(jnp.int32)
    rank = jnp.sum(hit[:, None, :] * earlier[None], -1)
    slots = jnp.arange(CAP * CORES, dtype=jnp.int32)
    chosen = hit[:, None, :] * (rank[:, None, :] == slots[None, :, None]).astype(jnp.int32)
    pids = jnp.sum(chosen * (ids % per_chip)[:, None, :], -1)
    blocks = jnp.sum(chosen * (order // NPB + 1)[None, None, :], -1) - 1
    blocks = jnp.where(blocks < 0, -CHUNK, blocks)
    return pids.reshape(-1), blocks.reshape(-1)


def body(
    tokens, ret_query, ret_key, ret_value, w_query, w_key, w_value, w_gate, store, passage_ids
):
    head_rank = lax.axis_index("tp")
    groups = w_query.shape[1] // HEAD_DIM
    token_count = tokens.shape[0]
    passages, rows, features = store.shape
    pids, blocks = slot_tables(passage_ids, passages * CORES)
    retained = retain(ret_query, ret_key, ret_value, head_rank * groups)
    whole = lax.all_gather(tokens, "tp", axis=1, tiled=True)
    queries = jnp.dot(whole, w_query, preferred_element_type=jnp.float32).astype(jnp.bfloat16)
    queries = queries.reshape(token_count // CHUNK, CHUNK, HEAD_DIM).transpose(0, 2, 1)
    gate_sum = jnp.dot(whole, w_gate, preferred_element_type=jnp.float32)
    gate_vals = jax.nn.sigmoid(lax.dynamic_slice_in_dim(gate_sum, head_rank * groups, groups, 1))
    keys = jnp.dot(store, w_key, preferred_element_type=jnp.float32).astype(jnp.bfloat16)
    values = jnp.dot(store, w_value, preferred_element_type=jnp.float32).astype(jnp.bfloat16)
    summed, stats = ring_attend(pids, blocks, queries, keys, values.transpose(0, 2, 1))
    gate_rows = gate_vals.reshape(token_count // CHUNK, 1, CHUNK)
    result = gate_rows * summed / stats[:, 1:2]
    retrieved = result.astype(jnp.bfloat16).transpose(0, 2, 1).reshape(token_count, groups, HEAD_DIM)
    return jnp.concatenate([retained, retrieved], -1).reshape(
        token_count, groups * (RET_DIM + HEAD_DIM)
    )


def solution(mesh):
    placed = (
        P(("grp", "st"), "tp"),
        P(("grp", "st"), "tp"),
        P(("grp", "st"), "tp"),
        P(("grp", "st"), "tp"),
        P(None, "tp"),
        P(None, "tp"),
        P(None, "tp"),
        P(),
        P("st", None, None),
        P(("grp", "st"), None),
    )
    return jax.shard_map(
        body, mesh=mesh, in_specs=placed, out_specs=P(("grp", "st"), "tp"), check_vma=False
    )
```

```python
import math

import jax
import jax.numpy as jnp
import numpy as np
from jax import lax
from jax.experimental import pallas as pl
from jax.experimental.pallas import tpu as pltpu
from jax.sharding import PartitionSpec as P

RET_DIM = 256
HEAD_DIM = 512
BLOCK = 64
NPB = 4
SEQ_LEN = 256
CAP = 2
CORES = 2
CHUNK = 128
ROTARY_BASE = 10000.0
NORM_EPS = 1e-05
MASKED = -1e30
FLOOR = -1e28
KV_PARTS = 2


def rotary_tables():
    halfway = RET_DIM // 2
    inverse = np.float32(ROTARY_BASE) ** (-np.arange(halfway, dtype=np.float32) / np.float32(halfway))
    angles = np.arange(SEQ_LEN, dtype=np.float32)[:, None] * inverse.astype(np.float32)
    return np.cos(angles).astype(np.float32), np.sin(angles).astype(np.float32)


def mixer_kernel(
    ids_ref, tokens_hbm, rq_hbm, rk_hbm, rv_hbm, wq_hbm, wk_hbm, wv_hbm, wg_hbm, store_hbm, cos_hbm, sin_hbm,
    out_ref,
    tbuf, wq, wk, wv, wg, store, rq, rk, rv, cosines, sines,
    ids_s, pid_s, blk_s, ids_in, qown, gate, qbuf, kall, vall, loc, locml, loc0, loc0ml, rbuf, rml,
    in_sem, ids_sem, t_sem, kv_send, kv_recv, x_send, x_recv, m_send, m_recv, q_send, q_recv,
    r_send, r_recv, s_send, s_recv,
):
    devices = lax.axis_size("st")
    ring = devices // CORES
    far = ring // 2
    chunks = qown.shape[0]
    half = chunks // 2
    slots = CAP * CORES
    mine = lax.axis_index("st")
    place, core = mine // CORES, mine % CORES
    right = lax.rem(mine + CORES, devices)
    left = lax.rem(mine + devices - CORES, devices)
    partner = mine + 1 - 2 * core
    toward = (right, left)
    xs = lax.axis_size("tp")
    head = lax.axis_index("tp")
    x_right, x_left = lax.rem(head + 1, xs), lax.rem(head + xs - 1, xs)
    x_toward = (x_right, x_left)
    x_source = (head, x_left, x_right, lax.rem(head + 2, xs))
    far_set = (tuple(range(0, chunks, 2)), tuple(range(1, chunks, 2)))
    send_order = (far_set[0] + far_set[1], far_set[1] + far_set[0])
    passages = kall.shape[1]
    rows = kall.shape[2]
    width = tokens_hbm.shape[1]
    ways = range(2)

    loads = [
        pltpu.make_async_copy(source, target, in_sem.at[i])
        for i, (source, target) in enumerate(
            (
                (store_hbm, store), (wk_hbm, wk), (wv_hbm, wv), (wq_hbm, wq), (wg_hbm, wg),
                (rq_hbm, rq), (rk_hbm, rk), (rv_hbm, rv), (cos_hbm, cosines), (sin_hbm, sines),
            )
        )
    ]
    token_loads = [
        pltpu.make_async_copy(tokens_hbm.at[pl.ds(j * CHUNK, CHUNK)], tbuf.at[j, 0], t_sem.at[j])
        for j in range(chunks)
    ]
    for copy in loads[:5]:
        copy.start()
    for copy in token_loads:
        copy.start()

    barrier = pltpu.get_barrier_semaphore()
    for device in (right, left, partner):
        pl.semaphore_signal(barrier, inc=1, device_id={"st": device})
    for device in x_toward:
        pl.semaphore_signal(barrier, inc=1, device_id={"tp": device})
    pl.semaphore_wait(barrier, 5)

    def x_copy(way, hop, j):
        if hop == 1:
            source, target = tokens_hbm.at[pl.ds(j * CHUNK, CHUNK)], tbuf.at[j, 1 + way]
        else:
            part = pl.ds(way * (CHUNK // 2), CHUNK // 2)
            source, target = tbuf.at[j, 1 + way, part], tbuf.at[j, 3, part]
        return pltpu.make_async_remote_copy(
            src_ref=source,
            dst_ref=target,
            send_sem=x_send.at[way, hop - 1, j],
            recv_sem=x_recv.at[way, hop - 1, j],
            device_id={"tp": x_toward[way]},
        )

    def is_first(hop):
        return isinstance(hop, int) and hop == 1

    def m_copy(way, hop):
        source = ids_ref if is_first(hop) else ids_in.at[way, jnp.maximum(hop - 2, 0)]
        return pltpu.make_async_remote_copy(
            src_ref=source,
            dst_ref=ids_in.at[way, hop - 1],
            send_sem=m_send.at[way, hop - 1],
            recv_sem=m_recv.at[way, hop - 1],
            device_id={"st": toward[way]},
        )

    def q_copy(way, hop, j):
        source = qown.at[j] if is_first(hop) else qbuf.at[way, jnp.maximum(hop - 2, 0), j]
        return pltpu.make_async_remote_copy(
            src_ref=source,
            dst_ref=qbuf.at[way, hop - 1, j],
            send_sem=q_send.at[way, hop - 1, j],
            recv_sem=q_recv.at[way, hop - 1, j],
            device_id={"st": toward[way]},
        )

    def kv_copy(i):
        everyone = (kall, vall)[i]
        return pltpu.make_async_remote_copy(
            src_ref=everyone.at[core],
            dst_ref=everyone.at[core],
            send_sem=kv_send.at[i],
            recv_sem=kv_recv.at[i],
            device_id={"st": partner},
        )

    def r_copies(way, hop, j):
        data = pltpu.make_async_remote_copy(
            src_ref=loc.at[1 - way, hop - 1, j],
            dst_ref=rbuf.at[way, hop - 1, j],
            send_sem=r_send.at[way, hop - 1, j],
            recv_sem=r_recv.at[way, hop - 1, j],
            device_id={"st": toward[way]},
        )
        stats = pltpu.make_async_remote_copy(
            src_ref=locml.at[1 - way, hop - 1, j],
            dst_ref=rml.at[way, hop - 1, j],
            send_sem=s_send.at[way, hop - 1, j],
            recv_sem=s_recv.at[way, hop - 1, j],
            device_id={"st": toward[way]},
        )
        return data, stats

    def fill_slots(source_row, table):
        fetch = pltpu.make_async_copy(source_row, ids_s.at[table], ids_sem)
        fetch.start()
        fetch.wait()
        lowest = place * (passages * CORES)

        def step(r, state):
            found, pids, blocks = state[0], state[1 : 1 + slots], state[1 + slots :]
            offset = ids_s[table, 0, r] - lowest
            hit = jnp.logical_and(offset >= 0, offset < passages * CORES)
            here = [jnp.logical_and(hit, found == s) for s in range(slots)]
            pids = tuple(jnp.where(h, offset, p) for h, p in zip(here, pids))
            blocks = tuple(jnp.where(h, r // NPB, b) for h, b in zip(here, blocks))
            return (found + jnp.where(hit, 1, 0),) + pids + blocks

        zero = jnp.int32(0)
        state = (zero,) + (zero,) * slots + (jnp.int32(-CHUNK),) * slots
        requests = chunks * (CHUNK // BLOCK) * NPB
        state = lax.fori_loop(0, requests, step, state)
        for s in range(slots):
            pid_s[table * slots + s] = state[1 + s]
            blk_s[table * slots + s] = state[1 + slots + s]

    lanes = lax.broadcasted_iota(jnp.int32, (1, CHUNK), 1)

    def attend(query, table, j):
        base = table * slots
        keys, values, penalties = [], [], []
        for slot in range(slots):
            passage = pid_s[base + slot]
            block = blk_s[base + slot]
            keys.append(kall[passage // passages, passage % passages])
            values.append(vall[passage // passages, passage % passages])
            within = block - j * (CHUNK // BLOCK)
            penalties.append(jnp.where(lanes // BLOCK == within, 0.0, MASKED))
        scores = [
            jnp.dot(key, query, preferred_element_type=jnp.float32) * HEAD_DIM ** (-0.5) + penalty
            for key, penalty in zip(keys, penalties)
        ]
        highest = jnp.full((1, CHUNK), FLOOR, jnp.float32)
        for score in scores:
            highest = jnp.maximum(highest, jnp.max(score, 0, keepdims=True))
        exponents = [jnp.exp(score - highest) for score in scores]
        total = jnp.zeros((1, CHUNK), jnp.float32)
        for exponent in exponents:
            total = total + jnp.sum(exponent, 0, keepdims=True)
        weighted = jnp.dot(
            jnp.concatenate(values, 1),
            jnp.concatenate([e.astype(jnp.bfloat16) for e in exponents], 0),
            preferred_element_type=jnp.float32,
        )
        return weighted, highest, total

    def attend_hop(hop, ways_chunks):
        for way, j in ways_chunks:
            weighted, highest, total = attend(qbuf[way, hop - 1, j], way * far + hop - 1, j)
            loc[way, hop - 1, j] = weighted.astype(jnp.bfloat16)
            locml[way, hop - 1, j, 0:1] = highest
            locml[way, hop - 1, j, 1:2] = total

    def project(j):
        total = jnp.zeros((CHUNK, HEAD_DIM), jnp.float32)
        logits = jnp.zeros((CHUNK, wg.shape[1]), jnp.float32)
        for r in range(4):
            features = pl.ds(pl.multiple_of(x_source[r] * width, width), width)
            part = tbuf[j, r]
            total = total + jnp.dot(part, wq[features], preferred_element_type=jnp.float32)
            logits = logits + jnp.dot(part, wg[features], preferred_element_type=jnp.float32)
        qown[j] = total.T.astype(jnp.bfloat16)
        columns = lax.broadcasted_iota(jnp.int32, logits.shape, 1)
        logit = jnp.sum(jnp.where(columns == head, logits, 0.0), 1, keepdims=True)
        gate[j] = jax.nn.sigmoid(logit)

    def make_keys(part):
        count = passages // KV_PARTS
        part_rows = store[pl.ds(part * count * rows, count * rows)]
        made = jnp.dot(part_rows, wk[...], preferred_element_type=jnp.float32).astype(jnp.bfloat16)
        for i in range(count):
            kall[core, part * count + i] = made[i * rows : (i + 1) * rows]

    def make_values(part):
        count = passages // KV_PARTS
        part_rows = store[pl.ds(part * count * rows, count * rows)]
        made = jnp.dot(part_rows, wv[...], preferred_element_type=jnp.float32)
        for i in range(count):
            vall[core, part * count + i] = made[i * rows : (i + 1) * rows].T.astype(jnp.bfloat16)

    def retention(sequence):
        span = pl.ds(sequence * SEQ_LEN, SEQ_LEN)
        halfway = RET_DIM // 2

        def turned(values, scale):
            leading = values[:, :halfway].astype(jnp.float32)
            trailing = values[:, halfway:].astype(jnp.float32)
            c, s = cosines[...], sines[...]
            both = jnp.concatenate([leading * c - trailing * s, leading * s + trailing * c], 1)
            return (both * scale if scale != 1.0 else both).astype(jnp.bfloat16)

        log_gamma = jnp.float32(0.0)
        for h in range(xs):
            log_gamma = jnp.where(head == h, jnp.float32(math.log1p(-(2.0 ** (-5 - h)))), log_gamma)
        grid = (SEQ_LEN, SEQ_LEN)
        offsets = lax.broadcasted_iota(jnp.int32, grid, 0) - lax.broadcasted_iota(jnp.int32, grid, 1)
        distance = jnp.maximum(offsets, 0).astype(jnp.float32)
        decays = jnp.where(offsets >= 0, jnp.exp(log_gamma * distance), 0.0)
        scores = lax.dot_general(
            turned(rq[span], 1.0), turned(rk[span], RET_DIM ** (-0.5)),
            (((1,), (1,)), ((), ())), preferred_element_type=jnp.float32,
        )
        raw = jnp.dot((scores * decays).astype(jnp.bfloat16), rv[span], preferred_element_type=jnp.float32)
        centred = raw - jnp.mean(raw, -1, keepdims=True)
        normed = centred * lax.rsqrt(jnp.mean(centred * centred, -1, keepdims=True) + NORM_EPS)
        out_ref[span, 0:RET_DIM] = normed.astype(jnp.bfloat16)

    def merge(first, first_ml, second, second_ml):
        top = jnp.maximum(first_ml[0], second_ml[0])
        left_scale, right_scale = jnp.exp(first_ml[0] - top), jnp.exp(second_ml[0] - top)
        summed = first * left_scale + second * right_scale
        total = first_ml[1] * left_scale + second_ml[1] * right_scale
        return summed, (top, total)

    for j in range(2):
        for way in ways:
            x_copy(way, 1, j).start()
    for way in ways:
        m_copy(way, 1).start()

    def x_forward(j):
        for way in ways:
            x_copy(way, 1, j).wait_recv()
            x_copy(way, 2, j).start()
            if j + 2 < chunks:
                x_copy(way, 1, j + 2).start()

    def q_make(j):
        token_loads[j].wait()
        for way in ways:
            x_copy(way, 2, j).wait_recv()
        project(j)

    def q_send_first(j):
        for way in ways:
            q_copy(way, 1, j).start()

    def arrive(hop, j, forward=True):
        for way in ways:
            q_copy(way, hop, j).wait_recv()
            if forward:
                q_copy(way, hop + 1, j).start()

    def m_arrive(hop, forward):
        for way in ways:
            m_copy(way, hop).wait_recv()
            if forward:
                m_copy(way, hop + 1).start()
        for way in ways:
            fill_slots(ids_in.at[way, hop - 1], way * far + hop - 1)

    loads[0].wait()
    loads[1].wait()
    make_keys(0)
    x_forward(0)
    make_keys(1)
    loads[2].wait()
    x_forward(1)
    make_values(0)
    kv_copy(0).start()
    loads[3].wait()
    loads[4].wait()
    q_make(0)
    x_forward(2)
    q_send_first(0)
    make_values(1)
    q_make(1)
    x_forward(3)
    q_send_first(1)
    kv_copy(1).start()
    fill_slots(ids_ref, 2 * far)
    m_arrive(1, far > 1)
    for copy in loads[5:]:
        copy.start()
    q_make(2)
    if far > 2:
        arrive(1, 0)
    q_send_first(2)
    q_make(3)
    if far > 2:
        arrive(1, 1)
    q_send_first(3)
    for i in range(2):
        kv_copy(i).wait()

    @pl.loop(0, chunks)
    def _(j):
        weighted, highest, total = attend(qown[j], 2 * far, j)
        loc0[j] = weighted.astype(jnp.bfloat16)
        loc0ml[j, 0:1] = highest
        loc0ml[j, 1:2] = total

    def attend_all(hop):
        @pl.loop(0, chunks)
        def _(j):
            attend_hop(hop, [(0, j), (1, j)])

    if far > 2:
        arrive(1, 2)
        arrive(1, 3)
        attend_all(1)

        @pl.loop(2, far - 2)
        def _(hop):
            m_arrive(hop, True)
            for j in range(chunks):
                arrive(hop, j)
            attend_all(hop)

        hop = far - 2
        m_arrive(hop, True)
        sent = [[], []]
        for j in range(chunks):
            arrive(hop, j, False)
            for way in ways:
                for chunk in send_order[way][len(sent[way]) : chunks - 1]:
                    if chunk > j:
                        break
                    q_copy(way, hop + 1, chunk).start()
                    sent[way].append(chunk)
        attend_all(hop)
        m_arrive(far - 1, True)
    for i in range(half):
        for way in ways:
            q_copy(way, far - 1, send_order[way][i]).wait_recv()
            q_copy(way, far, send_order[way][i]).start()
    if far > 2:
        for way in ways:
            q_copy(way, far - 1, send_order[way][chunks - 1]).start()
    for i in range(half):
        attend_hop(far - 1, [(way, send_order[way][i]) for way in ways])
    for i in range(half, chunks):
        for way in ways:
            q_copy(way, far - 1, send_order[way][i]).wait_recv()
        attend_hop(far - 1, [(way, send_order[way][i]) for way in ways])
    m_arrive(far, False)
    for i in range(half):
        for way in ways:
            q_copy(way, far, far_set[way][i]).wait_recv()
        attend_hop(far, [(way, far_set[way][i]) for way in ways])

    def r_start(way, hop, j):
        for copy in r_copies(way, hop, j):
            copy.start()

    def r_merge(way, hop, j):
        for copy in r_copies(way, hop + 1, j):
            copy.wait_recv()
        summed, (top, total) = merge(
            rbuf[way, hop, j].astype(jnp.float32),
            (rml[way, hop, j, 0:1], rml[way, hop, j, 1:2]),
            loc[1 - way, hop - 1, j].astype(jnp.float32),
            (locml[1 - way, hop - 1, j, 0:1], locml[1 - way, hop - 1, j, 1:2]),
        )
        loc[1 - way, hop - 1, j] = summed.astype(jnp.bfloat16)
        locml[1 - way, hop - 1, j, 0:1] = top
        locml[1 - way, hop - 1, j, 1:2] = total

    for i in range(half):
        for way in ways:
            r_start(way, far, far_set[1 - way][i])
    for i in range(half):
        for way in ways:
            r_start(way, far - 1, far_set[way][i])

    for copy in loads[5:]:
        copy.wait()
    retention(0)
    for i in range(half):
        for way in ways:
            r_merge(way, far - 1, far_set[1 - way][i])
        for way in ways:
            r_start(way, far - 1, far_set[1 - way][i])
    retention(1)

    @pl.loop(1, far - 1)
    def _(step):
        hop = far - 1 - step
        for j in range(chunks):
            for way in ways:
                r_merge(way, hop, send_order[way][j])
            for way in ways:
                r_start(way, hop, send_order[way][j])

    done = [set(), set()]
    for i in range(chunks):
        for way in ways:
            for copy in r_copies(way, 1, send_order[way][i]):
                copy.wait_recv()
            done[way].add(send_order[way][i])

    @pl.loop(0, chunks)
    def _(j):
        summed, both = loc0[j].astype(jnp.float32), (loc0ml[j, 0:1], loc0ml[j, 1:2])
        for way in ways:
            summed, both = merge(
                summed, both, rbuf[way, 0, j].astype(jnp.float32), (rml[way, 0, j, 0:1], rml[way, 0, j, 1:2])
            )
        share = (summed / both[1]).T * gate[j]
        out_ref[pl.ds(pl.multiple_of(j * CHUNK, CHUNK), CHUNK), RET_DIM:] = share.astype(jnp.bfloat16)

    for j in range(chunks):
        for way in ways:
            for hop in (1, 2):
                x_copy(way, hop, j).wait_send()
            q_copy(way, 1, j).wait_send()
    for way in ways:
        m_copy(way, 1).wait_send()

    @pl.loop(2, far + 1)
    def _(hop):
        for way in ways:
            m_copy(way, hop).wait_send()

    @pl.loop(2, far)
    def _(hop):
        for j in range(chunks):
            for way in ways:
                q_copy(way, hop, j).wait_send()

    @pl.loop(1, far)
    def _(hop):
        for j in range(chunks):
            for way in ways:
                for copy in r_copies(way, hop, j):
                    copy.wait_send()

    for way in ways:
        for j in far_set[way]:
            q_copy(way, far, j).wait_send()
        for j in far_set[1 - way]:
            for copy in r_copies(way, far, j):
                copy.wait_send()


def body(
    tokens, ret_query, ret_key, ret_value, w_query, w_key, w_value, w_gate, store, passage_ids
):
    ring = lax.axis_size("st") // CORES
    far = ring // 2
    xs = lax.axis_size("tp")
    token_count, width = tokens.shape
    chunks = token_count // CHUNK
    passages, rows, features = store.shape
    slots = CAP * CORES
    assert xs == 4 and w_query.shape[1] == HEAD_DIM and passages % KV_PARTS == 0
    ids = jnp.pad(passage_ids.reshape(1, -1), ((0, 0), (0, 128 - passage_ids.size)))
    cosines, sines = rotary_tables()
    buffer = (2, far, chunks, HEAD_DIM, CHUNK)
    stats = (2, far, chunks, 2, CHUNK)
    flags = (2, far, chunks)
    dma = pltpu.SemaphoreType.DMA
    bf16, f32, i32 = jnp.bfloat16, jnp.float32, jnp.int32
    hbm = pl.BlockSpec(memory_space=pl.ANY)
    vmem = pl.BlockSpec(memory_space=pltpu.VMEM)
    return pl.pallas_call(
        mixer_kernel,
        out_shape=jax.ShapeDtypeStruct((token_count, RET_DIM + HEAD_DIM), bf16),
        in_specs=[vmem] + [hbm] * 11,
        out_specs=vmem,
        scratch_shapes=[
            pltpu.VMEM((chunks, 4, CHUNK, width), bf16),
            pltpu.VMEM(w_query.shape, bf16),
            pltpu.VMEM(w_key.shape, bf16),
            pltpu.VMEM(w_value.shape, bf16),
            pltpu.VMEM(w_gate.shape, bf16),
            pltpu.VMEM((passages * rows, features), bf16),
            pltpu.VMEM(ret_query.shape, bf16),
            pltpu.VMEM(ret_query.shape, bf16),
            pltpu.VMEM(ret_query.shape, bf16),
            pltpu.VMEM(cosines.shape, f32),
            pltpu.VMEM(sines.shape, f32),
            pltpu.SMEM((2 * far + 1, 1, 128), i32),
            pltpu.SMEM(((2 * far + 1) * slots,), i32),
            pltpu.SMEM(((2 * far + 1) * slots,), i32),
            pltpu.VMEM((2, far, 1, 128), i32),
            pltpu.VMEM(buffer[2:], bf16),
            pltpu.VMEM((chunks, CHUNK, 1), f32),
            pltpu.VMEM(buffer, bf16),
            pltpu.VMEM((CORES, passages, rows, HEAD_DIM), bf16),
            pltpu.VMEM((CORES, passages, HEAD_DIM, rows), bf16),
            pltpu.VMEM(buffer, bf16),
            pltpu.VMEM(stats, f32),
            pltpu.VMEM(buffer[2:], bf16),
            pltpu.VMEM(stats[2:], f32),
            pltpu.VMEM(buffer, bf16),
            pltpu.VMEM(stats, f32),
            dma((10,)),
            dma,
            dma((chunks,)),
            dma((2,)),
            dma((2,)),
            dma((2, 2, chunks)),
            dma((2, 2, chunks)),
            dma((2, far)),
            dma((2, far)),
            dma(flags),
            dma(flags),
            dma(flags),
            dma(flags),
            dma(flags),
            dma(flags),
        ],
        compiler_params=pltpu.CompilerParams(
            collective_id=0, has_side_effects=True, vmem_limit_bytes=60 * 1024 * 1024
        ),
    )(
        ids, tokens, ret_query, ret_key, ret_value, w_query, w_key, w_value, w_gate,
        store.reshape(passages * rows, features), jnp.asarray(cosines), jnp.asarray(sines),
    )


def solution(mesh):
    placed = (
        P(("grp", "st"), "tp"),
        P(("grp", "st"), "tp"),
        P(("grp", "st"), "tp"),
        P(("grp", "st"), "tp"),
        P(None, "tp"),
        P(None, "tp"),
        P(None, "tp"),
        P(),
        P("st", None, None),
        P(("grp", "st"), None),
    )
    return jax.shard_map(
        body, mesh=mesh, in_specs=placed, out_specs=P(("grp", "st"), "tp"), check_vma=False
    )
```

```python
import math

import jax
import jax.numpy as jnp
import numpy as np
from jax import lax
from jax.experimental import pallas as pl
from jax.experimental.pallas import tpu as pltpu
from jax.sharding import PartitionSpec as P

RET_DIM = 256
HEAD_DIM = 512
BLOCK = 64
NPB = 4
SEQ_LEN = 256
CAP = 2
CORES = 2
CHUNK = 128
ROTARY_BASE = 10000.0
NORM_EPS = 1e-05
MASKED = -1e30
FLOOR = -1e28
PIECE = 64
KV_PARTS = 3


def rotary_tables():
    halfway = RET_DIM // 2
    inverse = np.float32(ROTARY_BASE) ** (-np.arange(halfway, dtype=np.float32) / np.float32(halfway))
    angles = np.arange(SEQ_LEN, dtype=np.float32)[:, None] * inverse.astype(np.float32)
    return np.cos(angles).astype(np.float32), np.sin(angles).astype(np.float32)


def mixer_kernel(
    ids_ref, tokens_hbm, rq_hbm, rk_hbm, rv_hbm, wq_hbm, wk_hbm, wv_hbm, wg_hbm, store_hbm, cos_hbm, sin_hbm,
    out_ref,
    tbuf, wq, wk, wv, wg, store, rq, rk, rv, cosines, sines,
    ids_s, pid_s, blk_s, ids_flat, ids_row, ids_in, qown, gate, qbuf, kall, vall, loc, locml, loc0, loc0ml, rbuf, rml,
    in_sem, ids_sem, t_sem, kv_send, kv_recv, x_send, x_recv, m_send, m_recv, q_send, q_recv,
    r_send, r_recv, s_send, s_recv,
):
    devices = lax.axis_size("st")
    ring = devices // CORES
    far = ring // 2
    chunks = qown.shape[0]
    half = chunks // 2
    slots = CAP * CORES
    mine = lax.axis_index("st")
    place, core = mine // CORES, mine % CORES
    right = lax.rem(mine + CORES, devices)
    left = lax.rem(mine + devices - CORES, devices)
    partner = mine + 1 - 2 * core
    toward = (right, left)
    xs = lax.axis_size("tp")
    head = lax.axis_index("tp")
    x_right, x_left = lax.rem(head + 1, xs), lax.rem(head + xs - 1, xs)
    x_toward = (x_right, x_left)
    x_source = (head, x_left, x_right, lax.rem(head + 2, xs))
    far_set = (tuple(range(0, chunks, 2)), tuple(range(1, chunks, 2)))
    send_order = (far_set[0] + far_set[1], far_set[1] + far_set[0])
    block_count = chunks * (CHUNK // BLOCK)
    pieces = chunks * (CHUNK // PIECE)
    passages = kall.shape[1]
    rows = kall.shape[2]
    width = tokens_hbm.shape[1]
    ways = range(2)

    loads = [
        pltpu.make_async_copy(source, target, in_sem.at[i])
        for i, (source, target) in enumerate(
            (
                (store_hbm, store), (wk_hbm, wk), (wv_hbm, wv), (wq_hbm, wq), (wg_hbm, wg),
                (rq_hbm, rq), (rk_hbm, rk), (rv_hbm, rv), (cos_hbm, cosines), (sin_hbm, sines),
            )
        )
    ]
    token_loads = [
        pltpu.make_async_copy(tokens_hbm.at[pl.ds(j * CHUNK, CHUNK)], tbuf.at[j, 0], t_sem.at[j])
        for j in range(chunks)
    ]
    for copy in loads[:5]:
        copy.start()
    for copy in token_loads:
        copy.start()

    barrier = pltpu.get_barrier_semaphore()
    for device in (right, left, partner):
        pl.semaphore_signal(barrier, inc=1, device_id={"st": device})
    for device in x_toward:
        pl.semaphore_signal(barrier, inc=1, device_id={"tp": device})
    pl.semaphore_wait(barrier, 5)

    def x_copy(way, hop, piece):
        j, first = divmod(piece * PIECE, CHUNK)
        if hop == 1:
            source = tokens_hbm.at[pl.ds(piece * PIECE, PIECE)]
            target = tbuf.at[j, 1 + way, pl.ds(first, PIECE)]
        else:
            part = pl.ds(first + way * (PIECE // 2), PIECE // 2)
            source, target = tbuf.at[j, 1 + way, part], tbuf.at[j, 3, part]
        return pltpu.make_async_remote_copy(
            src_ref=source,
            dst_ref=target,
            send_sem=x_send.at[way, hop - 1, piece],
            recv_sem=x_recv.at[way, hop - 1, piece],
            device_id={"tp": x_toward[way]},
        )

    def is_first(hop):
        return isinstance(hop, int) and hop == 1

    def m_copy(way, hop):
        source = ids_row if is_first(hop) else ids_in.at[way, jnp.maximum(hop - 2, 0)]
        return pltpu.make_async_remote_copy(
            src_ref=source,
            dst_ref=ids_in.at[way, hop - 1],
            send_sem=m_send.at[way, hop - 1],
            recv_sem=m_recv.at[way, hop - 1],
            device_id={"st": toward[way]},
        )

    def q_copy(way, hop, j):
        source = qown.at[j] if is_first(hop) else qbuf.at[way, jnp.maximum(hop - 2, 0), j]
        return pltpu.make_async_remote_copy(
            src_ref=source,
            dst_ref=qbuf.at[way, hop - 1, j],
            send_sem=q_send.at[way, hop - 1, j],
            recv_sem=q_recv.at[way, hop - 1, j],
            device_id={"st": toward[way]},
        )

    def kv_copy(i):
        everyone = (kall, vall)[i]
        return pltpu.make_async_remote_copy(
            src_ref=everyone.at[core],
            dst_ref=everyone.at[core],
            send_sem=kv_send.at[i],
            recv_sem=kv_recv.at[i],
            device_id={"st": partner},
        )

    def r_copies(way, hop, j):
        data = pltpu.make_async_remote_copy(
            src_ref=loc.at[1 - way, hop - 1, j],
            dst_ref=rbuf.at[way, hop - 1, j],
            send_sem=r_send.at[way, hop - 1, j],
            recv_sem=r_recv.at[way, hop - 1, j],
            device_id={"st": toward[way]},
        )
        stats = pltpu.make_async_remote_copy(
            src_ref=locml.at[1 - way, hop - 1, j],
            dst_ref=rml.at[way, hop - 1, j],
            send_sem=s_send.at[way, hop - 1, j],
            recv_sem=s_recv.at[way, hop - 1, j],
            device_id={"st": toward[way]},
        )
        return data, stats

    def fetch_ids(source_row, table):
        return pltpu.make_async_copy(source_row, ids_s.at[table], ids_sem.at[table])

    def fill_slots(table):
        lowest = place * (passages * CORES)

        def step(r, state):
            found, pids, blocks = state[0], state[1 : 1 + slots], state[1 + slots :]
            offset = ids_s[table, 0, r] - lowest
            hit = jnp.logical_and(offset >= 0, offset < passages * CORES)
            here = [jnp.logical_and(hit, found == s) for s in range(slots)]
            pids = tuple(jnp.where(h, offset, p) for h, p in zip(here, pids))
            blocks = tuple(jnp.where(h, lax.rem(r, block_count), b) for h, b in zip(here, blocks))
            return (found + jnp.where(hit, 1, 0),) + pids + blocks

        zero = jnp.int32(0)
        state = (zero,) + (zero,) * slots + (jnp.int32(-CHUNK),) * slots
        state = lax.fori_loop(0, block_count * NPB, step, state)
        for s in range(slots):
            pid_s[table * slots + s] = state[1 + s]
            blk_s[table * slots + s] = state[1 + slots + s]

    lanes = lax.broadcasted_iota(jnp.int32, (1, CHUNK), 1)

    def attend(query, table, j):
        base = table * slots
        keys, values, penalties = [], [], []
        for slot in range(slots):
            passage = pid_s[base + slot]
            block = blk_s[base + slot]
            keys.append(kall[passage // passages, passage % passages])
            values.append(vall[passage // passages, passage % passages])
            within = block - j * (CHUNK // BLOCK)
            penalties.append(jnp.where(lanes // BLOCK == within, 0.0, MASKED))
        scores = [
            jnp.dot(key, query, preferred_element_type=jnp.float32) * HEAD_DIM ** (-0.5) + penalty
            for key, penalty in zip(keys, penalties)
        ]
        highest = jnp.full((1, CHUNK), FLOOR, jnp.float32)
        for score in scores:
            highest = jnp.maximum(highest, jnp.max(score, 0, keepdims=True))
        exponents = [jnp.exp(score - highest) for score in scores]
        total = jnp.zeros((1, CHUNK), jnp.float32)
        for exponent in exponents:
            total = total + jnp.sum(exponent, 0, keepdims=True)
        weighted = jnp.dot(
            jnp.concatenate(values, 1),
            jnp.concatenate([e.astype(jnp.bfloat16) for e in exponents], 0),
            preferred_element_type=jnp.float32,
        )
        return weighted, highest, total

    def attend_hop(hop, ways_chunks):
        for way, j in ways_chunks:
            weighted, highest, total = attend(qbuf[way, hop - 1, j], way * far + hop - 1, j)
            loc[way, hop - 1, j] = weighted.astype(jnp.bfloat16)
            locml[way, hop - 1, j, 0:1] = highest
            locml[way, hop - 1, j, 1:2] = total

    def project(j):
        total = jnp.zeros((CHUNK, HEAD_DIM), jnp.float32)
        logits = jnp.zeros((wg.shape[0], CHUNK), jnp.float32)
        for r in range(4):
            features = pl.ds(pl.multiple_of(x_source[r] * width, width), width)
            part = tbuf[j, r]
            total = total + jnp.dot(part, wq[features], preferred_element_type=jnp.float32)
        qown[j] = total.T.astype(jnp.bfloat16)
        for r in range(4):
            features = pl.ds(pl.multiple_of(x_source[r] * width, width), width)
            logits = logits + lax.dot_general(
                wg[:, features], tbuf[j, r], (((1,), (1,)), ((), ())), preferred_element_type=jnp.float32
            )
        heads = lax.broadcasted_iota(jnp.int32, logits.shape, 0)
        logit = jnp.sum(jnp.where(heads == head, logits, 0.0), 0, keepdims=True)
        gate[j] = jax.nn.sigmoid(logit)

    def make_keys(part):
        count = passages // KV_PARTS
        part_rows = store[pl.ds(part * count * rows, count * rows)]
        made = jnp.dot(part_rows, wk[...], preferred_element_type=jnp.float32).astype(jnp.bfloat16)
        for i in range(count):
            kall[core, part * count + i] = made[i * rows : (i + 1) * rows]

    def make_values(part):
        count = passages // KV_PARTS
        part_rows = store[pl.ds(part * count * rows, count * rows)]
        made = jnp.dot(part_rows, wv[...], preferred_element_type=jnp.float32)
        for i in range(count):
            vall[core, part * count + i] = made[i * rows : (i + 1) * rows].T.astype(jnp.bfloat16)

    def retention(sequence):
        span = pl.ds(sequence * SEQ_LEN, SEQ_LEN)
        halfway = RET_DIM // 2

        def turned(values, scale):
            leading = values[:, :halfway].astype(jnp.float32)
            trailing = values[:, halfway:].astype(jnp.float32)
            c, s = cosines[...], sines[...]
            both = jnp.concatenate([leading * c - trailing * s, leading * s + trailing * c], 1)
            return (both * scale if scale != 1.0 else both).astype(jnp.bfloat16)

        log_gamma = jnp.float32(0.0)
        for h in range(xs):
            log_gamma = jnp.where(head == h, jnp.float32(math.log1p(-(2.0 ** (-5 - h)))), log_gamma)
        grid = (SEQ_LEN, SEQ_LEN)
        offsets = lax.broadcasted_iota(jnp.int32, grid, 0) - lax.broadcasted_iota(jnp.int32, grid, 1)
        distance = jnp.maximum(offsets, 0).astype(jnp.float32)
        decays = jnp.where(offsets >= 0, jnp.exp(log_gamma * distance), 0.0)
        scores = lax.dot_general(
            turned(rq[span], 1.0), turned(rk[span], RET_DIM ** (-0.5)),
            (((1,), (1,)), ((), ())), preferred_element_type=jnp.float32,
        )
        raw = jnp.dot((scores * decays).astype(jnp.bfloat16), rv[span], preferred_element_type=jnp.float32)
        centred = raw - jnp.mean(raw, -1, keepdims=True)
        normed = centred * lax.rsqrt(jnp.mean(centred * centred, -1, keepdims=True) + NORM_EPS)
        out_ref[span, 0:RET_DIM] = normed.astype(jnp.bfloat16)

    def merge(first, first_ml, second, second_ml):
        top = jnp.maximum(first_ml[0], second_ml[0])
        left_scale, right_scale = jnp.exp(first_ml[0] - top), jnp.exp(second_ml[0] - top)
        summed = first * left_scale + second * right_scale
        total = first_ml[1] * left_scale + second_ml[1] * right_scale
        return summed, (top, total)

    for piece in range(3):
        for way in ways:
            x_copy(way, 1, piece).start()
    ids_flat[...] = jnp.zeros_like(ids_flat)
    ids_flat[:, :block_count] = ids_ref[...]
    padded = ids_flat[...]
    row = padded[0:1]
    for slot in range(1, NPB):
        row = row + pltpu.roll(padded[slot : slot + 1], slot * block_count, 1)
    ids_row[...] = row

    def x_forward(piece):
        for way in ways:
            x_copy(way, 1, piece).wait_recv()
            x_copy(way, 2, piece).start()
            if 1 <= piece < pieces - 2:
                x_copy(way, 1, piece + 2).start()

    def q_make(j):
        token_loads[j].wait()
        for piece in range(j * (CHUNK // PIECE), (j + 1) * (CHUNK // PIECE)):
            for way in ways:
                x_copy(way, 2, piece).wait_recv()
        project(j)

    def q_send_first(j):
        for way in ways:
            q_copy(way, 1, j).start()

    def arrive(hop, j, forward=True):
        for way in ways:
            q_copy(way, hop, j).wait_recv()
            if forward:
                q_copy(way, hop + 1, j).start()

    def m_arrive(hop, forward):
        for way in ways:
            m_copy(way, hop).wait_recv()
            if forward:
                m_copy(way, hop + 1).start()
            fetch_ids(ids_in.at[way, hop - 1], way * far + hop - 1).start()

    def m_fill(hop):
        for way in ways:
            fetch_ids(ids_in.at[way, hop - 1], way * far + hop - 1).wait()
            fill_slots(way * far + hop - 1)

    loads[0].wait()
    loads[1].wait()
    make_keys(0)
    x_forward(0)
    for way in ways:
        m_copy(way, 1).start()
    fetch_ids(ids_row, 2 * far).start()
    make_keys(1)
    x_forward(1)
    make_keys(2)
    x_forward(2)
    loads[2].wait()
    make_values(0)
    loads[3].wait()
    loads[4].wait()
    kv_copy(0).start()
    q_make(0)
    x_forward(3)
    q_send_first(0)
    make_values(1)
    x_forward(4)
    q_make(1)
    x_forward(5)
    q_send_first(1)
    make_values(2)
    fetch_ids(ids_row, 2 * far).wait()
    fill_slots(2 * far)
    for copy in loads[5:]:
        copy.start()
    m_arrive(1, far > 1)
    if far > 2:
        arrive(1, 0)
    kv_copy(1).start()
    x_forward(6)
    q_make(2)
    m_fill(1)
    q_send_first(2)
    if far > 2:
        arrive(1, 1)
    x_forward(7)
    q_make(3)
    for i in range(2):
        kv_copy(i).wait()
    q_send_first(3)

    @pl.loop(0, chunks)
    def _(j):
        weighted, highest, total = attend(qown[j], 2 * far, j)
        loc0[j] = weighted.astype(jnp.bfloat16)
        loc0ml[j, 0:1] = highest
        loc0ml[j, 1:2] = total

    def attend_all(hop):
        @pl.loop(0, chunks)
        def _(j):
            attend_hop(hop, [(0, j), (1, j)])

    if far > 2:
        arrive(1, 2)
        arrive(1, 3)
        attend_all(1)

        @pl.loop(2, far - 2)
        def _(hop):
            m_arrive(hop, True)
            for j in range(chunks):
                arrive(hop, j)
            m_fill(hop)
            attend_all(hop)

        hop = far - 2
        m_arrive(hop, True)
        sent = [[], []]
        for j in range(chunks):
            arrive(hop, j, False)
            for way in ways:
                for chunk in send_order[way][len(sent[way]) : chunks - 1]:
                    if chunk > j:
                        break
                    q_copy(way, hop + 1, chunk).start()
                    sent[way].append(chunk)
        m_fill(hop)
        attend_all(hop)
        m_arrive(far - 1, True)
    for i in range(half):
        for way in ways:
            q_copy(way, far - 1, send_order[way][i]).wait_recv()
            q_copy(way, far, send_order[way][i]).start()
    if far > 2:
        for way in ways:
            q_copy(way, far - 1, send_order[way][chunks - 1]).start()
        m_fill(far - 1)

    def r_start(way, hop, j):
        for copy in r_copies(way, hop, j):
            copy.start()

    def r_merge(way, hop, j):
        for copy in r_copies(way, hop + 1, j):
            copy.wait_recv()
        summed, (top, total) = merge(
            rbuf[way, hop, j].astype(jnp.float32),
            (rml[way, hop, j, 0:1], rml[way, hop, j, 1:2]),
            loc[1 - way, hop - 1, j].astype(jnp.float32),
            (locml[1 - way, hop - 1, j, 0:1], locml[1 - way, hop - 1, j, 1:2]),
        )
        loc[1 - way, hop - 1, j] = summed.astype(jnp.bfloat16)
        locml[1 - way, hop - 1, j, 0:1] = top
        locml[1 - way, hop - 1, j, 1:2] = total

    for i in range(half):
        attend_hop(far - 1, [(way, send_order[way][i]) for way in ways])
    for way in ways:
        q_copy(way, far - 1, send_order[way][half]).wait_recv()
    attend_hop(far - 1, [(way, send_order[way][half]) for way in ways])
    m_arrive(far, False)
    m_fill(far)
    for i in range(half):
        for way in ways:
            q_copy(way, far, far_set[way][i]).wait_recv()
        attend_hop(far, [(way, far_set[way][i]) for way in ways])
        for way in ways:
            r_start(way, far, far_set[1 - way][i])
    for i in range(half):
        if i > 0:
            for way in ways:
                q_copy(way, far - 1, send_order[way][half + i]).wait_recv()
            attend_hop(far - 1, [(way, send_order[way][half + i]) for way in ways])
        for way in ways:
            r_start(way, far - 1, far_set[way][i])

    for copy in loads[5:]:
        copy.wait()
    retention(0)
    for i in range(half):
        for way in ways:
            r_merge(way, far - 1, far_set[1 - way][i])
        for way in ways:
            r_start(way, far - 1, far_set[1 - way][i])
    retention(1)

    @pl.loop(1, far - 1)
    def _(step):
        hop = far - 1 - step
        for j in range(chunks):
            for way in ways:
                r_merge(way, hop, send_order[way][j])
            for way in ways:
                r_start(way, hop, send_order[way][j])

    def finish(j):
        summed, both = loc0[j].astype(jnp.float32), (loc0ml[j, 0:1], loc0ml[j, 1:2])
        for way in ways:
            summed, both = merge(
                summed, both, rbuf[way, 0, j].astype(jnp.float32), (rml[way, 0, j, 0:1], rml[way, 0, j, 1:2])
            )
        share = (summed * (gate[j] / both[1])).T
        out_ref[j * CHUNK : (j + 1) * CHUNK, RET_DIM:] = share.astype(jnp.bfloat16)

    came = [set(), set()]
    for i in range(chunks):
        for way in ways:
            for copy in r_copies(way, 1, send_order[way][i]):
                copy.wait_recv()
        before = came[0] & came[1]
        for way in ways:
            came[way].add(send_order[way][i])
        for j in sorted((came[0] & came[1]) - before):
            finish(j)

    for j in range(chunks):
        for way in ways:
            q_copy(way, 1, j).wait_send()
    for way in ways:
        m_copy(way, 1).wait_send()
        for piece in range(pieces):
            for hop in (1, 2):
                x_copy(way, hop, piece).wait_send()

    @pl.loop(2, far + 1)
    def _(hop):
        for way in ways:
            m_copy(way, hop).wait_send()

    @pl.loop(2, far)
    def _(hop):
        for j in range(chunks):
            for way in ways:
                q_copy(way, hop, j).wait_send()

    @pl.loop(1, far)
    def _(hop):
        for j in range(chunks):
            for way in ways:
                for copy in r_copies(way, hop, j):
                    copy.wait_send()

    for way in ways:
        for j in far_set[way]:
            q_copy(way, far, j).wait_send()
        for j in far_set[1 - way]:
            for copy in r_copies(way, far, j):
                copy.wait_send()


def body(
    tokens, ret_query, ret_key, ret_value, w_query, w_key, w_value, w_gate, store, passage_ids
):
    ring = lax.axis_size("st") // CORES
    far = ring // 2
    xs = lax.axis_size("tp")
    token_count, width = tokens.shape
    chunks = token_count // CHUNK
    passages, rows, features = store.shape
    slots = CAP * CORES
    assert xs == 4 and w_query.shape[1] == HEAD_DIM and passages % KV_PARTS == 0
    assert passage_ids.size <= 128
    cosines, sines = rotary_tables()
    buffer = (2, far, chunks, HEAD_DIM, CHUNK)
    stats = (2, far, chunks, 2, CHUNK)
    flags = (2, far, chunks)
    dma = pltpu.SemaphoreType.DMA
    bf16, f32, i32 = jnp.bfloat16, jnp.float32, jnp.int32
    hbm = pl.BlockSpec(memory_space=pl.ANY)
    vmem = pl.BlockSpec(memory_space=pltpu.VMEM)
    return pl.pallas_call(
        mixer_kernel,
        out_shape=jax.ShapeDtypeStruct((token_count, RET_DIM + HEAD_DIM), bf16),
        in_specs=[vmem] + [hbm] * 11,
        out_specs=vmem,
        scratch_shapes=[
            pltpu.VMEM((chunks, 4, CHUNK, width), bf16),
            pltpu.VMEM(w_query.shape, bf16),
            pltpu.VMEM(w_key.shape, bf16),
            pltpu.VMEM(w_value.shape, bf16),
            pltpu.VMEM(w_gate.shape[::-1], bf16),
            pltpu.VMEM((passages * rows, features), bf16),
            pltpu.VMEM(ret_query.shape, bf16),
            pltpu.VMEM(ret_query.shape, bf16),
            pltpu.VMEM(ret_query.shape, bf16),
            pltpu.VMEM(cosines.shape, f32),
            pltpu.VMEM(sines.shape, f32),
            pltpu.SMEM((2 * far + 1, 1, 128), i32),
            pltpu.SMEM(((2 * far + 1) * slots,), i32),
            pltpu.SMEM(((2 * far + 1) * slots,), i32),
            pltpu.VMEM((NPB, 128), i32),
            pltpu.VMEM((1, 128), i32),
            pltpu.VMEM((2, far, 1, 128), i32),
            pltpu.VMEM(buffer[2:], bf16),
            pltpu.VMEM((chunks, 1, CHUNK), f32),
            pltpu.VMEM(buffer, bf16),
            pltpu.VMEM((CORES, passages, rows, HEAD_DIM), bf16),
            pltpu.VMEM((CORES, passages, HEAD_DIM, rows), bf16),
            pltpu.VMEM(buffer, bf16),
            pltpu.VMEM(stats, f32),
            pltpu.VMEM(buffer[2:], bf16),
            pltpu.VMEM(stats[2:], f32),
            pltpu.VMEM(buffer, bf16),
            pltpu.VMEM(stats, f32),
            dma((10,)),
            dma((2 * far + 1,)),
            dma((chunks,)),
            dma((2,)),
            dma((2,)),
            dma((2, 2, token_count // PIECE)),
            dma((2, 2, token_count // PIECE)),
            dma((2, far)),
            dma((2, far)),
            dma(flags),
            dma(flags),
            dma(flags),
            dma(flags),
            dma(flags),
            dma(flags),
        ],
        compiler_params=pltpu.CompilerParams(
            collective_id=0, has_side_effects=True, vmem_limit_bytes=60 * 1024 * 1024
        ),
    )(
        passage_ids.T, tokens, ret_query, ret_key, ret_value, w_query, w_key, w_value, w_gate.T,
        store.reshape(passages * rows, features), jnp.asarray(cosines), jnp.asarray(sines),
    )


def solution(mesh):
    placed = (
        P(("grp", "st"), "tp"),
        P(("grp", "st"), "tp"),
        P(("grp", "st"), "tp"),
        P(("grp", "st"), "tp"),
        P(None, "tp"),
        P(None, "tp"),
        P(None, "tp"),
        P(),
        P("st", None, None),
        P(("grp", "st"), None),
    )
    return jax.shard_map(
        body, mesh=mesh, in_specs=placed, out_specs=P(("grp", "st"), "tp"), check_vma=False
    )
```

```python
import math

import jax
import jax.numpy as jnp
import numpy as np
from jax import lax
from jax.experimental import pallas as pl
from jax.experimental.pallas import tpu as pltpu
from jax.sharding import PartitionSpec as P

RET_DIM = 256
HEAD_DIM = 512
BLOCK = 64
NPB = 4
SEQ_LEN = 256
CAP = 2
CORES = 2
CHUNK = 128
ROTARY_BASE = 10000.0
NORM_EPS = 1e-05
MASKED = -1e30
FLOOR = -1e28
PIECE = 64
KV_PARTS = 3


def rotary_tables():
    halfway = RET_DIM // 2
    inverse = np.float32(ROTARY_BASE) ** (-np.arange(halfway, dtype=np.float32) / np.float32(halfway))
    angles = np.arange(SEQ_LEN, dtype=np.float32)[:, None] * inverse.astype(np.float32)
    return np.cos(angles).astype(np.float32), np.sin(angles).astype(np.float32)


def mixer_kernel(
    ids_ref, tokens_hbm, rq_hbm, rk_hbm, rv_hbm, wq_hbm, wk_hbm, wv_hbm, wg_hbm, store_hbm, cos_hbm, sin_hbm,
    out_ref,
    tbuf, wq, wk, wv, wg, store, rq, rk, rv, cosines, sines,
    ids_s, pid_s, blk_s, ids_flat, ids_row, ids_in, qown, gate, qbuf, qlast_right, qlast_left, picked, kall, vall, loc, locml, loc0, loc0ml, rbuf, rml,
    in_sem, ids_sem, t_sem, kv_send, kv_recv, x_send, x_recv, m_send, m_recv, q_send, q_recv,
    r_send, r_recv, s_send, s_recv,
):
    devices = lax.axis_size("st")
    ring = devices // CORES
    far = ring // 2
    chunks = qown.shape[0]
    slots = CAP * CORES
    mine = lax.axis_index("st")
    place, core = mine // CORES, mine % CORES
    right = lax.rem(mine + CORES, devices)
    left = lax.rem(mine + devices - CORES, devices)
    partner = mine + 1 - 2 * core
    toward = (right, left)
    xs = lax.axis_size("tp")
    head = lax.axis_index("tp")
    x_right, x_left = lax.rem(head + 1, xs), lax.rem(head + xs - 1, xs)
    x_toward = (x_right, x_left)
    x_source = (head, x_left, x_right, lax.rem(head + 2, xs))
    block_count = chunks * (CHUNK // BLOCK)
    pieces = chunks * (CHUNK // PIECE)
    passages = kall.shape[1]
    rows = kall.shape[2]
    width = tokens_hbm.shape[1]
    ways = range(2)
    qlast = (qlast_right, qlast_left)
    relay = far - 2

    loads = [
        pltpu.make_async_copy(source, target, in_sem.at[i])
        for i, (source, target) in enumerate(
            (
                (store_hbm, store), (wk_hbm, wk), (wv_hbm, wv), (wq_hbm, wq), (wg_hbm, wg),
                (rq_hbm, rq), (rk_hbm, rk), (rv_hbm, rv), (cos_hbm, cosines), (sin_hbm, sines),
            )
        )
    ]
    token_loads = [
        pltpu.make_async_copy(tokens_hbm.at[pl.ds(j * CHUNK, CHUNK)], tbuf.at[j, 0], t_sem.at[j])
        for j in range(chunks)
    ]
    for copy in loads[:5]:
        copy.start()
    for copy in token_loads:
        copy.start()

    barrier = pltpu.get_barrier_semaphore()
    for device in (right, left, partner):
        pl.semaphore_signal(barrier, inc=1, device_id={"st": device})
    for device in x_toward:
        pl.semaphore_signal(barrier, inc=1, device_id={"tp": device})
    pl.semaphore_wait(barrier, 5)

    def x_copy(way, hop, piece):
        j, first = divmod(piece * PIECE, CHUNK)
        if hop == 1:
            source = tokens_hbm.at[pl.ds(piece * PIECE, PIECE)]
            target = tbuf.at[j, 1 + way, pl.ds(first, PIECE)]
        else:
            part = pl.ds(first + way * (PIECE // 2), PIECE // 2)
            source, target = tbuf.at[j, 1 + way, part], tbuf.at[j, 3, part]
        return pltpu.make_async_remote_copy(
            src_ref=source,
            dst_ref=target,
            send_sem=x_send.at[way, hop - 1, piece],
            recv_sem=x_recv.at[way, hop - 1, piece],
            device_id={"tp": x_toward[way]},
        )

    def is_first(hop):
        return isinstance(hop, int) and hop == 1

    def m_copy(way, hop):
        source = ids_row if is_first(hop) else ids_in.at[way, jnp.maximum(hop - 2, 0)]
        return pltpu.make_async_remote_copy(
            src_ref=source,
            dst_ref=ids_in.at[way, hop - 1],
            send_sem=m_send.at[way, hop - 1],
            recv_sem=m_recv.at[way, hop - 1],
            device_id={"st": toward[way]},
        )

    def q_copy(way, hop, j):
        static = isinstance(hop, int)
        if is_first(hop):
            source = qown.at[j]
        elif static and hop == relay + 1:
            source = picked.at[way, j]
        else:
            source = qbuf.at[way, jnp.maximum(hop - 2, 0), j]
        return pltpu.make_async_remote_copy(
            src_ref=source,
            dst_ref=qlast[way].at[j] if static and hop == relay else qbuf.at[way, hop - 1, j],
            send_sem=q_send.at[way, hop - 1, j],
            recv_sem=q_recv.at[way, hop - 1, j],
            device_id={"st": toward[way]},
        )

    def kv_copy(i):
        everyone = (kall, vall)[i]
        return pltpu.make_async_remote_copy(
            src_ref=everyone.at[core],
            dst_ref=everyone.at[core],
            send_sem=kv_send.at[i],
            recv_sem=kv_recv.at[i],
            device_id={"st": partner},
        )

    def r_copies(way, hop, j):
        passed_on = isinstance(hop, int) and hop == far - 1 and j == 0
        data = pltpu.make_async_remote_copy(
            src_ref=rbuf.at[way, hop, j] if passed_on else loc.at[1 - way, hop - 1, j],
            dst_ref=rbuf.at[way, hop - 1, j],
            send_sem=r_send.at[way, hop - 1, j],
            recv_sem=r_recv.at[way, hop - 1, j],
            device_id={"st": toward[way]},
        )
        stats = pltpu.make_async_remote_copy(
            src_ref=rml.at[way, hop, j] if passed_on else locml.at[1 - way, hop - 1, j],
            dst_ref=rml.at[way, hop - 1, j],
            send_sem=s_send.at[way, hop - 1, j],
            recv_sem=s_recv.at[way, hop - 1, j],
            device_id={"st": toward[way]},
        )
        return data, stats

    def fetch_ids(source_row, table):
        return pltpu.make_async_copy(source_row, ids_s.at[table], ids_sem.at[table])

    def fill_slots(ids, table, target):
        lowest = target * (passages * CORES)

        def step(r, state):
            found, pids, blocks = state[:CORES], state[CORES : CORES + slots], state[CORES + slots :]
            offset = ids_s[ids, 0, r] - lowest
            hits = [
                jnp.logical_and(offset >= c * passages, offset < (c + 1) * passages) for c in range(CORES)
            ]
            here = [jnp.logical_and(hits[s // CAP], found[s // CAP] == s % CAP) for s in range(slots)]
            pids = tuple(jnp.where(h, offset, p) for h, p in zip(here, pids))
            blocks = tuple(jnp.where(h, lax.rem(r, block_count), b) for h, b in zip(here, blocks))
            found = tuple(f + jnp.where(h, 1, 0) for f, h in zip(found, hits))
            return found + pids + blocks

        zero = jnp.int32(0)
        state = (zero,) * (CORES + slots) + (jnp.int32(-CHUNK),) * slots
        state = lax.fori_loop(0, block_count * NPB, step, state)
        for s in range(slots):
            pid_s[table * slots + s] = state[CORES + s]
            blk_s[table * slots + s] = state[CORES + slots + s]

    lanes = lax.broadcasted_iota(jnp.int32, (1, CHUNK), 1)

    def attend(query, table, j, pair=None):
        base = table * slots
        keys, values, penalties = [], [], []
        for slot in range(slots) if pair is None else range(pair * CAP, (pair + 1) * CAP):
            passage = pid_s[base + slot]
            block = blk_s[base + slot]
            keys.append(kall[passage // passages, passage % passages])
            values.append(vall[passage // passages, passage % passages])
            if pair is None:
                within = block - j * (CHUNK // BLOCK)
            else:
                within = jnp.where(block >= 0, slot % CAP, -1)
            penalties.append(jnp.where(lanes // BLOCK == within, 0.0, MASKED))
        scores = [
            jnp.dot(key, query, preferred_element_type=jnp.float32) * HEAD_DIM ** (-0.5) + penalty
            for key, penalty in zip(keys, penalties)
        ]
        highest = jnp.full((1, CHUNK), FLOOR, jnp.float32)
        for score in scores:
            highest = jnp.maximum(highest, jnp.max(score, 0, keepdims=True))
        exponents = [jnp.exp(score - highest) for score in scores]
        total = jnp.zeros((1, CHUNK), jnp.float32)
        for exponent in exponents:
            total = total + jnp.sum(exponent, 0, keepdims=True)
        weighted = jnp.dot(
            jnp.concatenate(values, 1),
            jnp.concatenate([e.astype(jnp.bfloat16) for e in exponents], 0),
            preferred_element_type=jnp.float32,
        )
        return weighted, highest, total

    def attend_hop(hop, ways_chunks):
        for way, j in ways_chunks:
            query = qlast[way][j] if isinstance(hop, int) and hop == relay else qbuf[way, hop - 1, j]
            weighted, highest, total = attend(query, way * far + hop - 1, j)
            loc[way, hop - 1, j] = weighted.astype(jnp.bfloat16)
            locml[way, hop - 1, j, 0:1] = highest
            locml[way, hop - 1, j, 1:2] = total

    def attend_pair(hop, way, j, pair):
        weighted, highest, total = attend(qbuf[way, hop - 1, j], way * far + hop - 1, j, pair)
        loc[way, hop - 1, j] = weighted.astype(jnp.bfloat16)
        locml[way, hop - 1, j, 0:1] = highest
        locml[way, hop - 1, j, 1:2] = total

    def beyond(way, j):
        return (2 * far + 2 + 2 * way, way) if j == 0 else (2 * far + 1 + 2 * way, j - 1)

    def fill_beyond(way):
        for away in (1, 2):
            target = lax.rem(place + (away if way == 0 else ring - away), ring)
            fill_slots(way * far + relay - 1, 2 * far + away + 2 * way, target)

    def pick(way, j):
        table, pair = beyond(way, j)
        parts = []
        for k in range(CAP):
            block = jnp.maximum(blk_s[table * slots + pair * CAP + k], 0)
            held = qlast[way][block // (CHUNK // BLOCK)].astype(jnp.float32)
            turned = pltpu.roll(held, BLOCK, 1)
            parts.append(jnp.where(block % (CHUNK // BLOCK) == k, held, turned))
        picked[way, j] = jnp.where(lanes < BLOCK, parts[0], parts[1]).astype(jnp.bfloat16)

    def project(j):
        total = jnp.zeros((CHUNK, HEAD_DIM), jnp.float32)
        logits = jnp.zeros((wg.shape[0], CHUNK), jnp.float32)
        for r in range(4):
            features = pl.ds(pl.multiple_of(x_source[r] * width, width), width)
            part = tbuf[j, r]
            total = total + jnp.dot(part, wq[features], preferred_element_type=jnp.float32)
        qown[j] = total.T.astype(jnp.bfloat16)
        for r in range(4):
            features = pl.ds(pl.multiple_of(x_source[r] * width, width), width)
            logits = logits + lax.dot_general(
                wg[:, features], tbuf[j, r], (((1,), (1,)), ((), ())), preferred_element_type=jnp.float32
            )
        heads = lax.broadcasted_iota(jnp.int32, logits.shape, 0)
        logit = jnp.sum(jnp.where(heads == head, logits, 0.0), 0, keepdims=True)
        gate[j] = jax.nn.sigmoid(logit)

    def make_keys(part):
        count = passages // KV_PARTS
        part_rows = store[pl.ds(part * count * rows, count * rows)]
        made = jnp.dot(part_rows, wk[...], preferred_element_type=jnp.float32).astype(jnp.bfloat16)
        for i in range(count):
            kall[core, part * count + i] = made[i * rows : (i + 1) * rows]

    def make_values(part):
        count = passages // KV_PARTS
        part_rows = store[pl.ds(part * count * rows, count * rows)]
        made = jnp.dot(part_rows, wv[...], preferred_element_type=jnp.float32)
        for i in range(count):
            vall[core, part * count + i] = made[i * rows : (i + 1) * rows].T.astype(jnp.bfloat16)

    def retention(sequence):
        span = pl.ds(sequence * SEQ_LEN, SEQ_LEN)
        halfway = RET_DIM // 2

        def turned(values, scale):
            leading = values[:, :halfway].astype(jnp.float32)
            trailing = values[:, halfway:].astype(jnp.float32)
            c, s = cosines[...], sines[...]
            both = jnp.concatenate([leading * c - trailing * s, leading * s + trailing * c], 1)
            return (both * scale if scale != 1.0 else both).astype(jnp.bfloat16)

        log_gamma = jnp.float32(0.0)
        for h in range(xs):
            log_gamma = jnp.where(head == h, jnp.float32(math.log1p(-(2.0 ** (-5 - h)))), log_gamma)
        grid = (SEQ_LEN, SEQ_LEN)
        offsets = lax.broadcasted_iota(jnp.int32, grid, 0) - lax.broadcasted_iota(jnp.int32, grid, 1)
        distance = jnp.maximum(offsets, 0).astype(jnp.float32)
        decays = jnp.where(offsets >= 0, jnp.exp(log_gamma * distance), 0.0)
        scores = lax.dot_general(
            turned(rq[span], 1.0), turned(rk[span], RET_DIM ** (-0.5)),
            (((1,), (1,)), ((), ())), preferred_element_type=jnp.float32,
        )
        raw = jnp.dot((scores * decays).astype(jnp.bfloat16), rv[span], preferred_element_type=jnp.float32)
        centred = raw - jnp.mean(raw, -1, keepdims=True)
        normed = centred * lax.rsqrt(jnp.mean(centred * centred, -1, keepdims=True) + NORM_EPS)
        out_ref[span, 0:RET_DIM] = normed.astype(jnp.bfloat16)

    def merge(first, first_ml, second, second_ml):
        top = jnp.maximum(first_ml[0], second_ml[0])
        left_scale, right_scale = jnp.exp(first_ml[0] - top), jnp.exp(second_ml[0] - top)
        summed = first * left_scale + second * right_scale
        total = first_ml[1] * left_scale + second_ml[1] * right_scale
        return summed, (top, total)

    for piece in range(3):
        for way in ways:
            x_copy(way, 1, piece).start()
    ids_flat[...] = jnp.zeros_like(ids_flat)
    ids_flat[:, :block_count] = ids_ref[...]
    padded = ids_flat[...]
    row = padded[0:1]
    for slot in range(1, NPB):
        row = row + pltpu.roll(padded[slot : slot + 1], slot * block_count, 1)
    ids_row[...] = row

    def x_forward(piece):
        for way in ways:
            x_copy(way, 1, piece).wait_recv()
            x_copy(way, 2, piece).start()
            if 1 <= piece < pieces - 2:
                x_copy(way, 1, piece + 2).start()

    def q_make(j):
        token_loads[j].wait()
        for piece in range(j * (CHUNK // PIECE), (j + 1) * (CHUNK // PIECE)):
            for way in ways:
                x_copy(way, 2, piece).wait_recv()
        project(j)

    def q_send_first(j):
        for way in ways:
            q_copy(way, 1, j).start()

    def arrive(hop, j, forward=True):
        for way in ways:
            q_copy(way, hop, j).wait_recv()
            if forward:
                q_copy(way, hop + 1, j).start()

    def m_arrive(hop, forward):
        for way in ways:
            m_copy(way, hop).wait_recv()
            if forward:
                m_copy(way, hop + 1).start()
            fetch_ids(ids_in.at[way, hop - 1], way * far + hop - 1).start()

    def m_fill(hop):
        for way in ways:
            fetch_ids(ids_in.at[way, hop - 1], way * far + hop - 1).wait()
            fill_slots(way * far + hop - 1, way * far + hop - 1, place)

    loads[0].wait()
    loads[1].wait()
    make_keys(0)
    x_forward(0)
    for way in ways:
        m_copy(way, 1).start()
    fetch_ids(ids_row, 2 * far).start()
    make_keys(1)
    x_forward(1)
    make_keys(2)
    x_forward(2)
    loads[2].wait()
    make_values(0)
    loads[3].wait()
    loads[4].wait()
    kv_copy(0).start()
    q_make(0)
    x_forward(3)
    q_send_first(0)
    make_values(1)
    x_forward(4)
    q_make(1)
    x_forward(5)
    q_send_first(1)
    make_values(2)
    fetch_ids(ids_row, 2 * far).wait()
    fill_slots(2 * far, 2 * far, place)
    for copy in loads[5:]:
        copy.start()
    m_arrive(1, True)
    arrive(1, 0)
    kv_copy(1).start()
    x_forward(6)
    q_make(2)
    m_fill(1)
    q_send_first(2)
    arrive(1, 1)
    x_forward(7)
    q_make(3)
    for i in range(2):
        kv_copy(i).wait()
    q_send_first(3)

    @pl.loop(0, chunks)
    def _(j):
        weighted, highest, total = attend(qown[j], 2 * far, j)
        loc0[j] = weighted.astype(jnp.bfloat16)
        loc0ml[j, 0:1] = highest
        loc0ml[j, 1:2] = total

    def attend_all(hop):
        @pl.loop(0, chunks)
        def _(j):
            attend_hop(hop, [(0, j), (1, j)])

    arrive(1, 2)
    arrive(1, 3)
    attend_all(1)

    @pl.loop(2, relay - 1)
    def _(hop):
        m_arrive(hop, True)
        for j in range(chunks):
            arrive(hop, j)
        m_fill(hop)
        attend_all(hop)

    if relay - 1 > 1:
        m_arrive(relay - 1, True)
        for j in range(chunks):
            arrive(relay - 1, j)
        m_fill(relay - 1)
        attend_all(relay - 1)

    m_arrive(relay, True)
    m_fill(relay)
    for way in ways:
        fill_beyond(way)
    for j in range(chunks):
        arrive(relay, j, False)
    for j in range(2):
        for way in ways:
            pick(way, j)
        for way in ways:
            q_copy(way, relay + 1, j).start()
    for way in ways:
        pick(way, 2)
    attend_hop(relay, [(way, 0) for way in ways])
    for way in ways:
        q_copy(way, relay + 1, 0).wait_recv()
        q_copy(way, far, 0).start()
    for way in ways:
        q_copy(way, relay + 1, 2).start()

    def r_start(way, hop, j):
        for copy in r_copies(way, hop, j):
            copy.start()

    def r_merge(way, hop, j):
        for copy in r_copies(way, hop + 1, j):
            copy.wait_recv()
        summed, (top, total) = merge(
            rbuf[way, hop, j].astype(jnp.float32),
            (rml[way, hop, j, 0:1], rml[way, hop, j, 1:2]),
            loc[1 - way, hop - 1, j].astype(jnp.float32),
            (locml[1 - way, hop - 1, j, 0:1], locml[1 - way, hop - 1, j, 1:2]),
        )
        loc[1 - way, hop - 1, j] = summed.astype(jnp.bfloat16)
        locml[1 - way, hop - 1, j, 0:1] = top
        locml[1 - way, hop - 1, j, 1:2] = total

    def r_scatter(way, j):
        data = [loc[1 - way, relay - 1, j].astype(jnp.float32)]
        tops = [locml[1 - way, relay - 1, j, 0:1]]
        totals = [locml[1 - way, relay - 1, j, 1:2]]
        valid = [None]
        for message in range(3):
            table, pair = beyond(1 - way, message)
            came = rbuf[way, relay, message].astype(jnp.float32)
            came_top, came_total = rml[way, relay, message, 0:1], rml[way, relay, message, 1:2]
            blocks = [blk_s[table * slots + pair * CAP + k] for k in range(CAP)]
            for shift in range(CAP):
                first, second = blocks[shift], blocks[1 - shift]
                wanted = jnp.where(lanes < BLOCK, first - j * CAP, second - j * CAP - 1) == 0
                if shift:
                    came, came_top, came_total = (
                        pltpu.roll(came, BLOCK, 1),
                        pltpu.roll(came_top, BLOCK, 1),
                        pltpu.roll(came_total, BLOCK, 1),
                    )
                data.append(came)
                tops.append(jnp.where(wanted, came_top, FLOOR))
                totals.append(came_total)
                valid.append(wanted)
        top = tops[0]
        for other in tops[1:]:
            top = jnp.maximum(top, other)
        summed, total = None, None
        for value, own_top, own_total, wanted in zip(data, tops, totals, valid):
            scale = jnp.exp(own_top - top)
            if wanted is None:
                summed, total = value * scale, own_total * scale
            else:
                scale = jnp.where(wanted, scale, 0.0)
                summed, total = summed + value * scale, total + own_total * scale
        loc[1 - way, relay - 1, j] = summed.astype(jnp.bfloat16)
        locml[1 - way, relay - 1, j, 0:1] = top
        locml[1 - way, relay - 1, j, 1:2] = total

    m_arrive(far - 1, True)

    @pl.loop(1, chunks)
    def _(j):
        attend_hop(relay, [(0, j), (1, j)])

    m_fill(far - 1)
    for way in ways:
        q_copy(way, far - 1, 1).wait_recv()
    for way in ways:
        attend_pair(far - 1, way, 1, 0)
    m_arrive(far, False)
    m_fill(far)
    for way in ways:
        q_copy(way, far, 0).wait_recv()
    for way in ways:
        attend_pair(far, way, 0, way)
    for way in ways:
        r_start(way, far, 0)
    for way in ways:
        r_start(way, far - 1, 1)
    for way in ways:
        q_copy(way, far - 1, 2).wait_recv()
    for way in ways:
        attend_pair(far - 1, way, 2, 1)
    for way in ways:
        for copy in r_copies(way, far, 0):
            copy.wait_recv()
        r_start(way, far - 1, 0)
    for way in ways:
        r_start(way, far - 1, 2)

    for copy in loads[5:]:
        copy.wait()
    retention(0)
    retention(1)

    for message in (1, 0, 2):
        for way in ways:
            for copy in r_copies(way, far - 1, message):
                copy.wait_recv()
    for j in range(chunks):
        for way in ways:
            r_scatter(way, j)
        for way in ways:
            r_start(way, relay, j)

    @pl.loop(1, relay)
    def _(step):
        hop = relay - step
        for j in range(chunks):
            for way in ways:
                r_merge(way, hop, j)
            for way in ways:
                r_start(way, hop, j)

    def finish(j):
        summed, both = loc0[j].astype(jnp.float32), (loc0ml[j, 0:1], loc0ml[j, 1:2])
        for way in ways:
            summed, both = merge(
                summed, both, rbuf[way, 0, j].astype(jnp.float32), (rml[way, 0, j, 0:1], rml[way, 0, j, 1:2])
            )
        share = (summed * (gate[j] / both[1])).T
        out_ref[j * CHUNK : (j + 1) * CHUNK, RET_DIM:] = share.astype(jnp.bfloat16)

    for j in range(chunks):
        for way in ways:
            for copy in r_copies(way, 1, j):
                copy.wait_recv()
        finish(j)

    for j in range(chunks):
        for way in ways:
            q_copy(way, 1, j).wait_send()
    for way in ways:
        m_copy(way, 1).wait_send()
        for piece in range(pieces):
            for hop in (1, 2):
                x_copy(way, hop, piece).wait_send()

    @pl.loop(2, far + 1)
    def _(hop):
        for way in ways:
            m_copy(way, hop).wait_send()

    @pl.loop(2, relay)
    def _(hop):
        for j in range(chunks):
            for way in ways:
                q_copy(way, hop, j).wait_send()

    @pl.loop(1, relay + 1)
    def _(hop):
        for j in range(chunks):
            for way in ways:
                for copy in r_copies(way, hop, j):
                    copy.wait_send()

    for way in ways:
        for j in range(chunks):
            q_copy(way, relay, j).wait_send()
        for hop, count in ((far - 1, 3), (far, 1)):
            for j in range(count):
                q_copy(way, hop, j).wait_send()
                for copy in r_copies(way, hop, j):
                    copy.wait_send()


def body(
    tokens, ret_query, ret_key, ret_value, w_query, w_key, w_value, w_gate, store, passage_ids
):
    ring = lax.axis_size("st") // CORES
    far = ring // 2
    xs = lax.axis_size("tp")
    token_count, width = tokens.shape
    chunks = token_count // CHUNK
    passages, rows, features = store.shape
    slots = CAP * CORES
    assert xs == 4 and far >= 4 and chunks == 4 and CHUNK == CAP * BLOCK and w_query.shape[1] == HEAD_DIM and passages % KV_PARTS == 0
    assert passage_ids.size <= 128
    cosines, sines = rotary_tables()
    buffer = (2, far, chunks, HEAD_DIM, CHUNK)
    stats = (2, far, chunks, 2, CHUNK)
    flags = (2, far, chunks)
    dma = pltpu.SemaphoreType.DMA
    bf16, f32, i32 = jnp.bfloat16, jnp.float32, jnp.int32
    hbm = pl.BlockSpec(memory_space=pl.ANY)
    vmem = pl.BlockSpec(memory_space=pltpu.VMEM)
    return pl.pallas_call(
        mixer_kernel,
        out_shape=jax.ShapeDtypeStruct((token_count, RET_DIM + HEAD_DIM), bf16),
        in_specs=[vmem] + [hbm] * 11,
        out_specs=vmem,
        scratch_shapes=[
            pltpu.VMEM((chunks, 4, CHUNK, width), bf16),
            pltpu.VMEM(w_query.shape, bf16),
            pltpu.VMEM(w_key.shape, bf16),
            pltpu.VMEM(w_value.shape, bf16),
            pltpu.VMEM(w_gate.shape[::-1], bf16),
            pltpu.VMEM((passages * rows, features), bf16),
            pltpu.VMEM(ret_query.shape, bf16),
            pltpu.VMEM(ret_query.shape, bf16),
            pltpu.VMEM(ret_query.shape, bf16),
            pltpu.VMEM(cosines.shape, f32),
            pltpu.VMEM(sines.shape, f32),
            pltpu.SMEM((2 * far + 1, 1, 128), i32),
            pltpu.SMEM(((2 * far + 5) * slots,), i32),
            pltpu.SMEM(((2 * far + 5) * slots,), i32),
            pltpu.VMEM((NPB, 128), i32),
            pltpu.VMEM((1, 128), i32),
            pltpu.VMEM((2, far, 1, 128), i32),
            pltpu.VMEM(buffer[2:], bf16),
            pltpu.VMEM((chunks, 1, CHUNK), f32),
            pltpu.VMEM(buffer, bf16),
            pltpu.VMEM(buffer[2:], bf16),
            pltpu.VMEM(buffer[2:], bf16),
            pltpu.VMEM((2, 3) + buffer[3:], bf16),
            pltpu.VMEM((CORES, passages, rows, HEAD_DIM), bf16),
            pltpu.VMEM((CORES, passages, HEAD_DIM, rows), bf16),
            pltpu.VMEM(buffer, bf16),
            pltpu.VMEM(stats, f32),
            pltpu.VMEM(buffer[2:], bf16),
            pltpu.VMEM(stats[2:], f32),
            pltpu.VMEM(buffer, bf16),
            pltpu.VMEM(stats, f32),
            dma((10,)),
            dma((2 * far + 1,)),
            dma((chunks,)),
            dma((2,)),
            dma((2,)),
            dma((2, 2, token_count // PIECE)),
            dma((2, 2, token_count // PIECE)),
            dma((2, far)),
            dma((2, far)),
            dma(flags),
            dma(flags),
            dma(flags),
            dma(flags),
            dma(flags),
            dma(flags),
        ],
        compiler_params=pltpu.CompilerParams(
            collective_id=0, has_side_effects=True, vmem_limit_bytes=60 * 1024 * 1024
        ),
    )(
        passage_ids.T, tokens, ret_query, ret_key, ret_value, w_query, w_key, w_value, w_gate.T,
        store.reshape(passages * rows, features), jnp.asarray(cosines), jnp.asarray(sines),
    )


def solution(mesh):
    placed = (
        P(("grp", "st"), "tp"),
        P(("grp", "st"), "tp"),
        P(("grp", "st"), "tp"),
        P(("grp", "st"), "tp"),
        P(None, "tp"),
        P(None, "tp"),
        P(None, "tp"),
        P(),
        P("st", None, None),
        P(("grp", "st"), None),
    )
    return jax.shard_map(
        body, mesh=mesh, in_specs=placed, out_specs=P(("grp", "st"), "tp"), check_vma=False
    )
```

```python
import math

import jax
import jax.numpy as jnp
import numpy as np
from jax import lax
from jax.experimental import pallas as pl
from jax.experimental.pallas import tpu as pltpu
from jax.sharding import PartitionSpec as P

RET_DIM = 256
HEAD_DIM = 512
BLOCK = 64
NPB = 4
SEQ_LEN = 256
CAP = 2
CORES = 2
CHUNK = 128
ROTARY_BASE = 10000.0
NORM_EPS = 1e-05
MASKED = -1e30
FLOOR = -1e28
PIECE = 64
KV_PARTS = 3


def rotary_tables():
    halfway = RET_DIM // 2
    inverse = np.float32(ROTARY_BASE) ** (-np.arange(halfway, dtype=np.float32) / np.float32(halfway))
    angles = np.arange(SEQ_LEN, dtype=np.float32)[:, None] * inverse.astype(np.float32)
    return np.cos(angles).astype(np.float32), np.sin(angles).astype(np.float32)


def mixer_kernel(
    ids_ref, tokens_hbm, rq_hbm, rk_hbm, rv_hbm, wq_hbm, wk_hbm, wv_hbm, wg_hbm, store_hbm, cos_hbm, sin_hbm,
    out_ref,
    tbuf, wq, wk, wv, wg, store, rq, rk, rv, cosines, sines,
    ids_s, pid_s, blk_s, ids_flat, ids_row, ids_in, qown, gate, qbuf, qlast_right, qlast_left, picked, kall, vall, loc, locml, loc0, loc0ml, rbuf, rml,
    in_sem, ids_sem, t_sem, kv_send, kv_recv, x_send, x_recv, m_send, m_recv, q_send, q_recv,
    r_send, r_recv, s_send, s_recv,
):
    devices = lax.axis_size("st")
    ring = devices // CORES
    far = ring // 2
    chunks = qown.shape[0]
    slots = CAP * CORES
    mine = lax.axis_index("st")
    place, core = mine // CORES, mine % CORES
    right = lax.rem(mine + CORES, devices)
    left = lax.rem(mine + devices - CORES, devices)
    partner = mine + 1 - 2 * core
    toward = (right, left)
    xs = lax.axis_size("tp")
    head = lax.axis_index("tp")
    x_right, x_left = lax.rem(head + 1, xs), lax.rem(head + xs - 1, xs)
    x_toward = (x_right, x_left)
    x_source = (head, x_left, x_right, lax.rem(head + 2, xs))
    block_count = chunks * (CHUNK // BLOCK)
    pieces = chunks * (CHUNK // PIECE)
    passages = kall.shape[1]
    rows = kall.shape[2]
    width = tokens_hbm.shape[1]
    ways = range(2)
    qlast = (qlast_right, qlast_left)
    relay = far - 2

    loads = [
        pltpu.make_async_copy(source, target, in_sem.at[i])
        for i, (source, target) in enumerate(
            (
                (store_hbm, store), (wk_hbm, wk), (wv_hbm, wv), (wq_hbm, wq), (wg_hbm, wg),
                (rq_hbm, rq), (rk_hbm, rk), (rv_hbm, rv), (cos_hbm, cosines), (sin_hbm, sines),
            )
        )
    ]
    token_loads = [
        pltpu.make_async_copy(tokens_hbm.at[pl.ds(j * CHUNK, CHUNK)], tbuf.at[j, 0], t_sem.at[j])
        for j in range(chunks)
    ]
    for copy in loads[:5]:
        copy.start()
    for copy in token_loads:
        copy.start()

    barrier = pltpu.get_barrier_semaphore()
    for device in (right, left, partner):
        pl.semaphore_signal(barrier, inc=1, device_id={"st": device})
    for device in x_toward:
        pl.semaphore_signal(barrier, inc=1, device_id={"tp": device})
    pl.semaphore_wait(barrier, 5)

    def x_copy(way, hop, piece):
        j, first = divmod(piece * PIECE, CHUNK)
        if hop == 1:
            source = tokens_hbm.at[pl.ds(piece * PIECE, PIECE)]
            target = tbuf.at[j, 1 + way, pl.ds(first, PIECE)]
        else:
            part = pl.ds(first + way * (PIECE // 2), PIECE // 2)
            source, target = tbuf.at[j, 1 + way, part], tbuf.at[j, 3, part]
        return pltpu.make_async_remote_copy(
            src_ref=source,
            dst_ref=target,
            send_sem=x_send.at[way, hop - 1, piece],
            recv_sem=x_recv.at[way, hop - 1, piece],
            device_id={"tp": x_toward[way]},
        )

    def is_first(hop):
        return isinstance(hop, int) and hop == 1

    def m_copy(way, hop):
        source = ids_row if is_first(hop) else ids_in.at[way, jnp.maximum(hop - 2, 0)]
        return pltpu.make_async_remote_copy(
            src_ref=source,
            dst_ref=ids_in.at[way, hop - 1],
            send_sem=m_send.at[way, hop - 1],
            recv_sem=m_recv.at[way, hop - 1],
            device_id={"st": toward[way]},
        )

    def q_copy(way, hop, j):
        static = isinstance(hop, int)
        if is_first(hop):
            source = qown.at[j]
        elif static and hop == relay + 1:
            source = picked.at[way, j]
        else:
            source = qbuf.at[way, jnp.maximum(hop - 2, 0), j]
        return pltpu.make_async_remote_copy(
            src_ref=source,
            dst_ref=qlast[way].at[j] if static and hop == relay else qbuf.at[way, hop - 1, j],
            send_sem=q_send.at[way, hop - 1, j],
            recv_sem=q_recv.at[way, hop - 1, j],
            device_id={"st": toward[way]},
        )

    def kv_copy(i):
        everyone = (kall, vall)[i]
        return pltpu.make_async_remote_copy(
            src_ref=everyone.at[core],
            dst_ref=everyone.at[core],
            send_sem=kv_send.at[i],
            recv_sem=kv_recv.at[i],
            device_id={"st": partner},
        )

    def r_copies(way, hop, j):
        passed_on = isinstance(hop, int) and hop == far - 1 and j == 0
        data = pltpu.make_async_remote_copy(
            src_ref=rbuf.at[way, hop, j] if passed_on else loc.at[1 - way, hop - 1, j],
            dst_ref=rbuf.at[way, hop - 1, j],
            send_sem=r_send.at[way, hop - 1, j],
            recv_sem=r_recv.at[way, hop - 1, j],
            device_id={"st": toward[way]},
        )
        stats = pltpu.make_async_remote_copy(
            src_ref=rml.at[way, hop, j] if passed_on else locml.at[1 - way, hop - 1, j],
            dst_ref=rml.at[way, hop - 1, j],
            send_sem=s_send.at[way, hop - 1, j],
            recv_sem=s_recv.at[way, hop - 1, j],
            device_id={"st": toward[way]},
        )
        return data, stats

    def fetch_ids(source_row, table):
        return pltpu.make_async_copy(source_row, ids_s.at[table], ids_sem.at[table])

    def fill_slots(ids, table, target):
        lowest = target * (passages * CORES)

        def step(r, state):
            found, pids, blocks = state[:CORES], state[CORES : CORES + slots], state[CORES + slots :]
            offset = ids_s[ids, 0, r] - lowest
            hits = [
                jnp.logical_and(offset >= c * passages, offset < (c + 1) * passages) for c in range(CORES)
            ]
            here = [jnp.logical_and(hits[s // CAP], found[s // CAP] == s % CAP) for s in range(slots)]
            pids = tuple(jnp.where(h, offset, p) for h, p in zip(here, pids))
            blocks = tuple(jnp.where(h, lax.rem(r, block_count), b) for h, b in zip(here, blocks))
            found = tuple(f + jnp.where(h, 1, 0) for f, h in zip(found, hits))
            return found + pids + blocks

        zero = jnp.int32(0)
        state = (zero,) * (CORES + slots) + (jnp.int32(-CHUNK),) * slots
        state = lax.fori_loop(0, block_count * NPB, step, state)
        for s in range(slots):
            pid_s[table * slots + s] = state[CORES + s]
            blk_s[table * slots + s] = state[CORES + slots + s]

    lanes = lax.broadcasted_iota(jnp.int32, (1, CHUNK), 1)

    def attend(query, table, j, pair=None):
        base = table * slots
        keys, values, penalties = [], [], []
        for slot in range(slots) if pair is None else range(pair * CAP, (pair + 1) * CAP):
            passage = pid_s[base + slot]
            block = blk_s[base + slot]
            keys.append(kall[passage // passages, passage % passages])
            values.append(vall[passage // passages, passage % passages])
            if pair is None:
                within = block - j * (CHUNK // BLOCK)
            else:
                within = jnp.where(block >= 0, slot % CAP, -1)
            penalties.append(jnp.where(lanes // BLOCK == within, 0.0, MASKED))
        scores = [
            jnp.dot(key, query, preferred_element_type=jnp.float32) * HEAD_DIM ** (-0.5) + penalty
            for key, penalty in zip(keys, penalties)
        ]
        highest = jnp.full((1, CHUNK), FLOOR, jnp.float32)
        for score in scores:
            highest = jnp.maximum(highest, jnp.max(score, 0, keepdims=True))
        exponents = [jnp.exp(score - highest) for score in scores]
        total = jnp.zeros((1, CHUNK), jnp.float32)
        for exponent in exponents:
            total = total + jnp.sum(exponent, 0, keepdims=True)
        weighted = jnp.dot(
            jnp.concatenate(values, 1),
            jnp.concatenate([e.astype(jnp.bfloat16) for e in exponents], 0),
            preferred_element_type=jnp.float32,
        )
        return weighted, highest, total

    def attend_hop(hop, ways_chunks):
        for way, j in ways_chunks:
            query = qlast[way][j] if isinstance(hop, int) and hop == relay else qbuf[way, hop - 1, j]
            weighted, highest, total = attend(query, way * far + hop - 1, j)
            loc[way, hop - 1, j] = weighted.astype(jnp.bfloat16)
            locml[way, hop - 1, j, 0:1] = highest
            locml[way, hop - 1, j, 1:2] = total

    def attend_pair(hop, way, j, pair):
        weighted, highest, total = attend(qbuf[way, hop - 1, j], way * far + hop - 1, j, pair)
        loc[way, hop - 1, j] = weighted.astype(jnp.bfloat16)
        locml[way, hop - 1, j, 0:1] = highest
        locml[way, hop - 1, j, 1:2] = total

    def beyond(way, j):
        return (2 * far + 2 + 2 * way, way) if j == 0 else (2 * far + 1 + 2 * way, j - 1)

    def fill_beyond(way):
        for away in (1, 2):
            target = lax.rem(place + (away if way == 0 else ring - away), ring)
            fill_slots(way * far + relay - 1, 2 * far + away + 2 * way, target)

    def pick(way, j):
        table, pair = beyond(way, j)
        parts = []
        for k in range(CAP):
            block = jnp.maximum(blk_s[table * slots + pair * CAP + k], 0)
            held = qlast[way][block // (CHUNK // BLOCK)].astype(jnp.float32)
            turned = pltpu.roll(held, BLOCK, 1)
            parts.append(jnp.where(block % (CHUNK // BLOCK) == k, held, turned))
        picked[way, j] = jnp.where(lanes < BLOCK, parts[0], parts[1]).astype(jnp.bfloat16)

    def project(j):
        total = jnp.zeros((CHUNK, HEAD_DIM), jnp.float32)
        logits = jnp.zeros((wg.shape[0], CHUNK), jnp.float32)
        for r in range(4):
            features = pl.ds(pl.multiple_of(x_source[r] * width, width), width)
            part = tbuf[j, r]
            total = total + jnp.dot(part, wq[features], preferred_element_type=jnp.float32)
        qown[j] = total.T.astype(jnp.bfloat16)
        for r in range(4):
            features = pl.ds(pl.multiple_of(x_source[r] * width, width), width)
            logits = logits + lax.dot_general(
                wg[:, features], tbuf[j, r], (((1,), (1,)), ((), ())), preferred_element_type=jnp.float32
            )
        heads = lax.broadcasted_iota(jnp.int32, logits.shape, 0)
        logit = jnp.sum(jnp.where(heads == head, logits, 0.0), 0, keepdims=True)
        gate[j] = jax.nn.sigmoid(logit)

    def make_keys(part):
        count = passages // KV_PARTS
        part_rows = store[pl.ds(part * count * rows, count * rows)]
        made = jnp.dot(part_rows, wk[...], preferred_element_type=jnp.float32).astype(jnp.bfloat16)
        for i in range(count):
            kall[core, part * count + i] = made[i * rows : (i + 1) * rows]

    def make_values(part):
        count = passages // KV_PARTS
        part_rows = store[pl.ds(part * count * rows, count * rows)]
        made = jnp.dot(part_rows, wv[...], preferred_element_type=jnp.float32)
        for i in range(count):
            vall[core, part * count + i] = made[i * rows : (i + 1) * rows].T.astype(jnp.bfloat16)

    def retention(sequence):
        span = pl.ds(sequence * SEQ_LEN, SEQ_LEN)
        halfway = RET_DIM // 2

        def turned(values, scale):
            leading = values[:, :halfway].astype(jnp.float32)
            trailing = values[:, halfway:].astype(jnp.float32)
            c, s = cosines[...], sines[...]
            both = jnp.concatenate([leading * c - trailing * s, leading * s + trailing * c], 1)
            return (both * scale if scale != 1.0 else both).astype(jnp.bfloat16)

        log_gamma = jnp.float32(0.0)
        for h in range(xs):
            log_gamma = jnp.where(head == h, jnp.float32(math.log1p(-(2.0 ** (-5 - h)))), log_gamma)
        grid = (SEQ_LEN, SEQ_LEN)
        offsets = lax.broadcasted_iota(jnp.int32, grid, 0) - lax.broadcasted_iota(jnp.int32, grid, 1)
        distance = jnp.maximum(offsets, 0).astype(jnp.float32)
        decays = jnp.where(offsets >= 0, jnp.exp(log_gamma * distance), 0.0)
        scores = lax.dot_general(
            turned(rq[span], 1.0), turned(rk[span], RET_DIM ** (-0.5)),
            (((1,), (1,)), ((), ())), preferred_element_type=jnp.float32,
        )
        raw = jnp.dot((scores * decays).astype(jnp.bfloat16), rv[span], preferred_element_type=jnp.float32)
        centred = raw - jnp.mean(raw, -1, keepdims=True)
        normed = centred * lax.rsqrt(jnp.mean(centred * centred, -1, keepdims=True) + NORM_EPS)
        out_ref[span, 0:RET_DIM] = normed.astype(jnp.bfloat16)

    def merge(first, first_ml, second, second_ml):
        top = jnp.maximum(first_ml[0], second_ml[0])
        left_scale, right_scale = jnp.exp(first_ml[0] - top), jnp.exp(second_ml[0] - top)
        summed = first * left_scale + second * right_scale
        total = first_ml[1] * left_scale + second_ml[1] * right_scale
        return summed, (top, total)

    for piece in range(3):
        for way in ways:
            x_copy(way, 1, piece).start()
    ids_flat[...] = jnp.zeros_like(ids_flat)
    ids_flat[:, :block_count] = ids_ref[...]
    padded = ids_flat[...]
    row = padded[0:1]
    for slot in range(1, NPB):
        row = row + pltpu.roll(padded[slot : slot + 1], slot * block_count, 1)
    ids_row[...] = row

    def x_forward(piece):
        for way in ways:
            x_copy(way, 1, piece).wait_recv()
            x_copy(way, 2, piece).start()
            if 1 <= piece < pieces - 2:
                x_copy(way, 1, piece + 2).start()

    def q_make(j):
        token_loads[j].wait()
        for piece in range(j * (CHUNK // PIECE), (j + 1) * (CHUNK // PIECE)):
            for way in ways:
                x_copy(way, 2, piece).wait_recv()
        project(j)

    def q_send_first(j):
        for way in ways:
            q_copy(way, 1, j).start()

    def arrive(hop, j, forward=True):
        for way in ways:
            q_copy(way, hop, j).wait_recv()
            if forward:
                q_copy(way, hop + 1, j).start()

    def m_arrive(hop, forward):
        for way in ways:
            m_copy(way, hop).wait_recv()
            if forward:
                m_copy(way, hop + 1).start()
            fetch_ids(ids_in.at[way, hop - 1], way * far + hop - 1).start()

    def m_fill(hop):
        for way in ways:
            fetch_ids(ids_in.at[way, hop - 1], way * far + hop - 1).wait()
            fill_slots(way * far + hop - 1, way * far + hop - 1, place)

    loads[0].wait()
    loads[1].wait()
    make_keys(0)
    x_forward(0)
    for way in ways:
        m_copy(way, 1).start()
    fetch_ids(ids_row, 2 * far).start()
    make_keys(1)
    x_forward(1)
    make_keys(2)
    x_forward(2)
    loads[2].wait()
    make_values(0)
    loads[3].wait()
    loads[4].wait()
    kv_copy(0).start()
    q_make(0)
    x_forward(3)
    q_send_first(0)
    make_values(1)
    x_forward(4)
    q_make(1)
    x_forward(5)
    q_send_first(1)
    make_values(2)
    fetch_ids(ids_row, 2 * far).wait()
    fill_slots(2 * far, 2 * far, place)
    for copy in loads[5:]:
        copy.start()
    m_arrive(1, True)
    arrive(1, 0)
    kv_copy(1).start()
    x_forward(6)
    q_make(2)
    m_fill(1)
    q_send_first(2)
    arrive(1, 1)
    x_forward(7)
    q_make(3)
    for i in range(2):
        kv_copy(i).wait()
    q_send_first(3)

    def attend_own(first):
        @pl.loop(first, first + 2)
        def _(j):
            weighted, highest, total = attend(qown[j], 2 * far, j)
            loc0[j] = weighted.astype(jnp.bfloat16)
            loc0ml[j, 0:1] = highest
            loc0ml[j, 1:2] = total

    def attend_both(hop, j):
        attend_hop(hop, [(way, j) for way in ways])

    def pass_hop(hop):
        m_arrive(hop, True)

        @pl.loop(0, chunks)
        def _(j):
            arrive(hop, j)
            attend_both(hop - 1, j)

        m_fill(hop)

    attend_own(0)
    arrive(1, 2)
    attend_own(2)
    m_arrive(2, True)

    @pl.loop(0, 2)
    def _(j):
        arrive(2, j, relay > 2)
        attend_both(1, j)

    arrive(1, 3)

    @pl.loop(2, chunks)
    def _(j):
        attend_both(1, j)
        arrive(2, j, relay > 2)

    m_fill(2)
    if relay > 3:

        @pl.loop(3, relay - 1)
        def _(hop):
            pass_hop(hop)

        pass_hop(relay - 1)
    if relay > 2:
        m_arrive(relay, True)
        m_fill(relay)
    for way in ways:
        fill_beyond(way)
    if relay > 2:

        @pl.loop(0, chunks - 1)
        def _(j):
            arrive(relay, j, False)
            attend_both(relay - 1, j)

        arrive(relay, chunks - 1, False)
    for j in range(2):
        for way in ways:
            pick(way, j)
        for way in ways:
            q_copy(way, relay + 1, j).start()
    for way in ways:
        pick(way, 2)
    if relay > 2:
        attend_both(relay - 1, chunks - 1)
    for way in ways:
        q_copy(way, relay + 1, 0).wait_recv()
        q_copy(way, far, 0).start()
    for way in ways:
        q_copy(way, relay + 1, 2).start()

    def r_start(way, hop, j):
        for copy in r_copies(way, hop, j):
            copy.start()

    def r_merge(way, hop, j):
        for copy in r_copies(way, hop + 1, j):
            copy.wait_recv()
        summed, (top, total) = merge(
            rbuf[way, hop, j].astype(jnp.float32),
            (rml[way, hop, j, 0:1], rml[way, hop, j, 1:2]),
            loc[1 - way, hop - 1, j].astype(jnp.float32),
            (locml[1 - way, hop - 1, j, 0:1], locml[1 - way, hop - 1, j, 1:2]),
        )
        loc[1 - way, hop - 1, j] = summed.astype(jnp.bfloat16)
        locml[1 - way, hop - 1, j, 0:1] = top
        locml[1 - way, hop - 1, j, 1:2] = total

    def r_scatter(way, j):
        data = [loc[1 - way, relay - 1, j].astype(jnp.float32)]
        tops = [locml[1 - way, relay - 1, j, 0:1]]
        totals = [locml[1 - way, relay - 1, j, 1:2]]
        valid = [None]
        for message in range(3):
            table, pair = beyond(1 - way, message)
            came = rbuf[way, relay, message].astype(jnp.float32)
            came_top, came_total = rml[way, relay, message, 0:1], rml[way, relay, message, 1:2]
            blocks = [blk_s[table * slots + pair * CAP + k] for k in range(CAP)]
            for shift in range(CAP):
                first, second = blocks[shift], blocks[1 - shift]
                wanted = jnp.where(lanes < BLOCK, first - j * CAP, second - j * CAP - 1) == 0
                if shift:
                    came, came_top, came_total = (
                        pltpu.roll(came, BLOCK, 1),
                        pltpu.roll(came_top, BLOCK, 1),
                        pltpu.roll(came_total, BLOCK, 1),
                    )
                data.append(came)
                tops.append(jnp.where(wanted, came_top, FLOOR))
                totals.append(came_total)
                valid.append(wanted)
        top = tops[0]
        for other in tops[1:]:
            top = jnp.maximum(top, other)
        summed, total = None, None
        for value, own_top, own_total, wanted in zip(data, tops, totals, valid):
            scale = jnp.exp(own_top - top)
            if wanted is None:
                summed, total = value * scale, own_total * scale
            else:
                scale = jnp.where(wanted, scale, 0.0)
                summed, total = summed + value * scale, total + own_total * scale
        loc[1 - way, relay - 1, j] = summed.astype(jnp.bfloat16)
        locml[1 - way, relay - 1, j, 0:1] = top
        locml[1 - way, relay - 1, j, 1:2] = total

    m_arrive(far - 1, True)

    @pl.loop(0, 2)
    def _(j):
        attend_both(relay, j)

    m_fill(far - 1)
    for way in ways:
        q_copy(way, far - 1, 1).wait_recv()
    for way in ways:
        attend_pair(far - 1, way, 1, 0)
    m_arrive(far, False)
    m_fill(far)
    for way in ways:
        q_copy(way, far, 0).wait_recv()
    for way in ways:
        attend_pair(far, way, 0, way)
    for way in ways:
        r_start(way, far, 0)
    for way in ways:
        r_start(way, far - 1, 1)
    for way in ways:
        q_copy(way, far - 1, 2).wait_recv()
    for way in ways:
        attend_pair(far - 1, way, 2, 1)
    for way in ways:
        for copy in r_copies(way, far, 0):
            copy.wait_recv()
        r_start(way, far - 1, 0)
    for way in ways:
        r_start(way, far - 1, 2)

    @pl.loop(2, chunks)
    def _(j):
        attend_both(relay, j)

    for copy in loads[5:]:
        copy.wait()
    retention(0)
    retention(1)

    for message in (1, 0, 2):
        for way in ways:
            for copy in r_copies(way, far - 1, message):
                copy.wait_recv()
    for j in range(chunks):
        for way in ways:
            r_scatter(way, j)
        for way in ways:
            r_start(way, relay, j)

    @pl.loop(1, relay)
    def _(step):
        hop = relay - step
        for j in range(chunks):
            for way in ways:
                r_merge(way, hop, j)
            for way in ways:
                r_start(way, hop, j)

    def finish(j):
        summed, both = loc0[j].astype(jnp.float32), (loc0ml[j, 0:1], loc0ml[j, 1:2])
        for way in ways:
            summed, both = merge(
                summed, both, rbuf[way, 0, j].astype(jnp.float32), (rml[way, 0, j, 0:1], rml[way, 0, j, 1:2])
            )
        share = (summed * (gate[j] / both[1])).T
        out_ref[j * CHUNK : (j + 1) * CHUNK, RET_DIM:] = share.astype(jnp.bfloat16)

    for j in range(chunks):
        for way in ways:
            for copy in r_copies(way, 1, j):
                copy.wait_recv()
        finish(j)

    for j in range(chunks):
        for way in ways:
            q_copy(way, 1, j).wait_send()
    for way in ways:
        m_copy(way, 1).wait_send()
        for piece in range(pieces):
            for hop in (1, 2):
                x_copy(way, hop, piece).wait_send()

    @pl.loop(2, far + 1)
    def _(hop):
        for way in ways:
            m_copy(way, hop).wait_send()

    @pl.loop(2, relay)
    def _(hop):
        for j in range(chunks):
            for way in ways:
                q_copy(way, hop, j).wait_send()

    @pl.loop(1, relay + 1)
    def _(hop):
        for j in range(chunks):
            for way in ways:
                for copy in r_copies(way, hop, j):
                    copy.wait_send()

    for way in ways:
        for j in range(chunks):
            q_copy(way, relay, j).wait_send()
        for hop, count in ((far - 1, 3), (far, 1)):
            for j in range(count):
                q_copy(way, hop, j).wait_send()
                for copy in r_copies(way, hop, j):
                    copy.wait_send()


def body(
    tokens, ret_query, ret_key, ret_value, w_query, w_key, w_value, w_gate, store, passage_ids
):
    ring = lax.axis_size("st") // CORES
    far = ring // 2
    xs = lax.axis_size("tp")
    token_count, width = tokens.shape
    chunks = token_count // CHUNK
    passages, rows, features = store.shape
    slots = CAP * CORES
    assert xs == 4 and far >= 4 and chunks == 4 and CHUNK == CAP * BLOCK and w_query.shape[1] == HEAD_DIM and passages % KV_PARTS == 0
    assert passage_ids.size <= 128
    cosines, sines = rotary_tables()
    buffer = (2, far, chunks, HEAD_DIM, CHUNK)
    stats = (2, far, chunks, 2, CHUNK)
    flags = (2, far, chunks)
    dma = pltpu.SemaphoreType.DMA
    bf16, f32, i32 = jnp.bfloat16, jnp.float32, jnp.int32
    hbm = pl.BlockSpec(memory_space=pl.ANY)
    vmem = pl.BlockSpec(memory_space=pltpu.VMEM)
    return pl.pallas_call(
        mixer_kernel,
        out_shape=jax.ShapeDtypeStruct((token_count, RET_DIM + HEAD_DIM), bf16),
        in_specs=[vmem] + [hbm] * 11,
        out_specs=vmem,
        scratch_shapes=[
            pltpu.VMEM((chunks, 4, CHUNK, width), bf16),
            pltpu.VMEM(w_query.shape, bf16),
            pltpu.VMEM(w_key.shape, bf16),
            pltpu.VMEM(w_value.shape, bf16),
            pltpu.VMEM(w_gate.shape[::-1], bf16),
            pltpu.VMEM((passages * rows, features), bf16),
            pltpu.VMEM(ret_query.shape, bf16),
            pltpu.VMEM(ret_query.shape, bf16),
            pltpu.VMEM(ret_query.shape, bf16),
            pltpu.VMEM(cosines.shape, f32),
            pltpu.VMEM(sines.shape, f32),
            pltpu.SMEM((2 * far + 1, 1, 128), i32),
            pltpu.SMEM(((2 * far + 5) * slots,), i32),
            pltpu.SMEM(((2 * far + 5) * slots,), i32),
            pltpu.VMEM((NPB, 128), i32),
            pltpu.VMEM((1, 128), i32),
            pltpu.VMEM((2, far, 1, 128), i32),
            pltpu.VMEM(buffer[2:], bf16),
            pltpu.VMEM((chunks, 1, CHUNK), f32),
            pltpu.VMEM(buffer, bf16),
            pltpu.VMEM(buffer[2:], bf16),
            pltpu.VMEM(buffer[2:], bf16),
            pltpu.VMEM((2, 3) + buffer[3:], bf16),
            pltpu.VMEM((CORES, passages, rows, HEAD_DIM), bf16),
            pltpu.VMEM((CORES, passages, HEAD_DIM, rows), bf16),
            pltpu.VMEM(buffer, bf16),
            pltpu.VMEM(stats, f32),
            pltpu.VMEM(buffer[2:], bf16),
            pltpu.VMEM(stats[2:], f32),
            pltpu.VMEM(buffer, bf16),
            pltpu.VMEM(stats, f32),
            dma((10,)),
            dma((2 * far + 1,)),
            dma((chunks,)),
            dma((2,)),
            dma((2,)),
            dma((2, 2, token_count // PIECE)),
            dma((2, 2, token_count // PIECE)),
            dma((2, far)),
            dma((2, far)),
            dma(flags),
            dma(flags),
            dma(flags),
            dma(flags),
            dma(flags),
            dma(flags),
        ],
        compiler_params=pltpu.CompilerParams(
            collective_id=0, has_side_effects=True, vmem_limit_bytes=60 * 1024 * 1024
        ),
    )(
        passage_ids.T, tokens, ret_query, ret_key, ret_value, w_query, w_key, w_value, w_gate.T,
        store.reshape(passages * rows, features), jnp.asarray(cosines), jnp.asarray(sines),
    )


def solution(mesh):
    placed = (
        P(("grp", "st"), "tp"),
        P(("grp", "st"), "tp"),
        P(("grp", "st"), "tp"),
        P(("grp", "st"), "tp"),
        P(None, "tp"),
        P(None, "tp"),
        P(None, "tp"),
        P(),
        P("st", None, None),
        P(("grp", "st"), None),
    )
    return jax.shard_map(
        body, mesh=mesh, in_specs=placed, out_specs=P(("grp", "st"), "tp"), check_vma=False
    )
```

```python
import math

import jax
import jax.numpy as jnp
import numpy as np
from jax import lax
from jax.experimental import pallas as pl
from jax.experimental.pallas import tpu as pltpu
from jax.sharding import PartitionSpec as P

RET_DIM = 256
HEAD_DIM = 512
BLOCK = 64
NPB = 4
SEQ_LEN = 256
CAP = 2
CORES = 2
CHUNK = 128
ROTARY_BASE = 10000.0
NORM_EPS = 1e-05
MASKED = -1e30
FLOOR = -1e28
PIECE = 64
KV_PARTS = 3


def rotary_tables():
    halfway = RET_DIM // 2
    inverse = np.float32(ROTARY_BASE) ** (-np.arange(halfway, dtype=np.float32) / np.float32(halfway))
    angles = np.arange(SEQ_LEN, dtype=np.float32)[:, None] * inverse.astype(np.float32)
    return np.cos(angles).astype(np.float32), np.sin(angles).astype(np.float32)


def mixer_kernel(
    ids_ref, tokens_hbm, rq_hbm, rk_hbm, rv_hbm, wq_hbm, wk_hbm, wv_hbm, wg_hbm, store_hbm, cos_hbm, sin_hbm,
    out_ref,
    tbuf, wq, wk, wv, wg, store, rq, rk, rv, cosines, sines,
    ids_s, pid_s, blk_s, ids_flat, ids_row, ids_in, qown, gate, qbuf, qlast_right, qlast_left, picked, kall, vall, loc, locml, loc0, loc0ml, rbuf, rml,
    in_sem, ids_sem, t_sem, kv_send, kv_recv, x_send, x_recv, m_send, m_recv, q_send, q_recv,
    r_send, r_recv, s_send, s_recv,
):
    devices = lax.axis_size("st")
    ring = devices // CORES
    far = ring // 2
    chunks = qown.shape[0]
    slots = CAP * CORES
    mine = lax.axis_index("st")
    place, core = mine // CORES, mine % CORES
    right = lax.rem(mine + CORES, devices)
    left = lax.rem(mine + devices - CORES, devices)
    partner = mine + 1 - 2 * core
    toward = (right, left)
    xs = lax.axis_size("tp")
    head = lax.axis_index("tp")
    x_right, x_left = lax.rem(head + 1, xs), lax.rem(head + xs - 1, xs)
    x_toward = (x_right, x_left)
    x_source = (head, x_left, x_right, lax.rem(head + 2, xs))
    block_count = chunks * (CHUNK // BLOCK)
    pieces = chunks * (CHUNK // PIECE)
    passages = kall.shape[1]
    rows = kall.shape[2]
    width = tokens_hbm.shape[1]
    ways = range(2)
    qlast = (qlast_right, qlast_left)
    relay = far - 2

    loads = [
        pltpu.make_async_copy(source, target, in_sem.at[i])
        for i, (source, target) in enumerate(
            (
                (store_hbm, store), (wk_hbm, wk), (wv_hbm, wv), (wq_hbm, wq), (wg_hbm, wg),
                (rq_hbm, rq), (rk_hbm, rk), (rv_hbm, rv), (cos_hbm, cosines), (sin_hbm, sines),
            )
        )
    ]
    token_loads = [
        pltpu.make_async_copy(tokens_hbm.at[pl.ds(j * CHUNK, CHUNK)], tbuf.at[j, 0], t_sem.at[j])
        for j in range(chunks)
    ]
    for copy in loads[:5]:
        copy.start()
    for copy in token_loads:
        copy.start()

    barrier = pltpu.get_barrier_semaphore()
    for device in (right, left, partner):
        pl.semaphore_signal(barrier, inc=1, device_id={"st": device})
    for device in x_toward:
        pl.semaphore_signal(barrier, inc=1, device_id={"tp": device})
    pl.semaphore_wait(barrier, 5)

    def x_copy(way, hop, piece):
        j, first = divmod(piece * PIECE, CHUNK)
        if hop == 1:
            source = tokens_hbm.at[pl.ds(piece * PIECE, PIECE)]
            target = tbuf.at[j, 1 + way, pl.ds(first, PIECE)]
        else:
            part = pl.ds(first + way * (PIECE // 2), PIECE // 2)
            source, target = tbuf.at[j, 1 + way, part], tbuf.at[j, 3, part]
        return pltpu.make_async_remote_copy(
            src_ref=source,
            dst_ref=target,
            send_sem=x_send.at[way, hop - 1, piece],
            recv_sem=x_recv.at[way, hop - 1, piece],
            device_id={"tp": x_toward[way]},
        )

    def is_first(hop):
        return isinstance(hop, int) and hop == 1

    def m_copy(way, hop):
        source = ids_row if is_first(hop) else ids_in.at[way, jnp.maximum(hop - 2, 0)]
        return pltpu.make_async_remote_copy(
            src_ref=source,
            dst_ref=ids_in.at[way, hop - 1],
            send_sem=m_send.at[way, hop - 1],
            recv_sem=m_recv.at[way, hop - 1],
            device_id={"st": toward[way]},
        )

    def q_copy(way, hop, j):
        static = isinstance(hop, int)
        if is_first(hop):
            source = qown.at[j]
        elif static and hop == relay + 1:
            source = picked.at[way, j]
        else:
            source = qbuf.at[way, jnp.maximum(hop - 2, 0), j]
        return pltpu.make_async_remote_copy(
            src_ref=source,
            dst_ref=qlast[way].at[j] if static and hop == relay else qbuf.at[way, hop - 1, j],
            send_sem=q_send.at[way, hop - 1, j],
            recv_sem=q_recv.at[way, hop - 1, j],
            device_id={"st": toward[way]},
        )

    def kv_copy(i):
        everyone = (kall, vall)[i]
        return pltpu.make_async_remote_copy(
            src_ref=everyone.at[core],
            dst_ref=everyone.at[core],
            send_sem=kv_send.at[i],
            recv_sem=kv_recv.at[i],
            device_id={"st": partner},
        )

    def r_copies(way, hop, j):
        passed_on = isinstance(hop, int) and hop == far - 1 and j == 0
        data = pltpu.make_async_remote_copy(
            src_ref=rbuf.at[way, hop, j] if passed_on else loc.at[1 - way, hop - 1, j],
            dst_ref=rbuf.at[way, hop - 1, j],
            send_sem=r_send.at[way, hop - 1, j],
            recv_sem=r_recv.at[way, hop - 1, j],
            device_id={"st": toward[way]},
        )
        stats = pltpu.make_async_remote_copy(
            src_ref=rml.at[way, hop, j] if passed_on else locml.at[1 - way, hop - 1, j],
            dst_ref=rml.at[way, hop - 1, j],
            send_sem=s_send.at[way, hop - 1, j],
            recv_sem=s_recv.at[way, hop - 1, j],
            device_id={"st": toward[way]},
        )
        return data, stats

    def fetch_ids(source_row, table):
        return pltpu.make_async_copy(source_row, ids_s.at[table], ids_sem.at[table])

    def fill_slots(ids, table, target):
        lowest = target * (passages * CORES)

        def step(r, state):
            found, pids, blocks = state[:CORES], state[CORES : CORES + slots], state[CORES + slots :]
            offset = ids_s[ids, 0, r] - lowest
            hits = [
                jnp.logical_and(offset >= c * passages, offset < (c + 1) * passages) for c in range(CORES)
            ]
            here = [jnp.logical_and(hits[s // CAP], found[s // CAP] == s % CAP) for s in range(slots)]
            pids = tuple(jnp.where(h, offset, p) for h, p in zip(here, pids))
            blocks = tuple(jnp.where(h, lax.rem(r, block_count), b) for h, b in zip(here, blocks))
            found = tuple(f + jnp.where(h, 1, 0) for f, h in zip(found, hits))
            return found + pids + blocks

        zero = jnp.int32(0)
        state = (zero,) * (CORES + slots) + (jnp.int32(-CHUNK),) * slots
        state = lax.fori_loop(0, block_count * NPB, step, state)
        for s in range(slots):
            pid_s[table * slots + s] = state[CORES + s]
            blk_s[table * slots + s] = state[CORES + slots + s]

    lanes = lax.broadcasted_iota(jnp.int32, (1, CHUNK), 1)

    def attend(query, table, j, pair=None):
        base = table * slots
        keys, values, penalties = [], [], []
        for slot in range(slots) if pair is None else range(pair * CAP, (pair + 1) * CAP):
            passage = pid_s[base + slot]
            block = blk_s[base + slot]
            keys.append(kall[passage // passages, passage % passages])
            values.append(vall[passage // passages, passage % passages])
            if pair is None:
                within = block - j * (CHUNK // BLOCK)
            else:
                within = jnp.where(block >= 0, slot % CAP, -1)
            penalties.append(jnp.where(lanes // BLOCK == within, 0.0, MASKED))
        scores = [
            jnp.dot(key, query, preferred_element_type=jnp.float32) * HEAD_DIM ** (-0.5) + penalty
            for key, penalty in zip(keys, penalties)
        ]
        highest = jnp.full((1, CHUNK), FLOOR, jnp.float32)
        for score in scores:
            highest = jnp.maximum(highest, jnp.max(score, 0, keepdims=True))
        exponents = [jnp.exp(score - highest) for score in scores]
        total = jnp.zeros((1, CHUNK), jnp.float32)
        for exponent in exponents:
            total = total + jnp.sum(exponent, 0, keepdims=True)
        weighted = jnp.dot(
            jnp.concatenate(values, 1),
            jnp.concatenate([e.astype(jnp.bfloat16) for e in exponents], 0),
            preferred_element_type=jnp.float32,
        )
        return weighted, highest, total

    def attend_hop(hop, ways_chunks):
        for way, j in ways_chunks:
            query = qlast[way][j] if isinstance(hop, int) and hop == relay else qbuf[way, hop - 1, j]
            weighted, highest, total = attend(query, way * far + hop - 1, j)
            loc[way, hop - 1, j] = weighted.astype(jnp.bfloat16)
            locml[way, hop - 1, j, 0:1] = highest
            locml[way, hop - 1, j, 1:2] = total

    def attend_pair(hop, way, j, pair):
        weighted, highest, total = attend(qbuf[way, hop - 1, j], way * far + hop - 1, j, pair)
        loc[way, hop - 1, j] = weighted.astype(jnp.bfloat16)
        locml[way, hop - 1, j, 0:1] = highest
        locml[way, hop - 1, j, 1:2] = total

    def beyond(way, j):
        return (2 * far + 2 + 2 * way, way) if j == 0 else (2 * far + 1 + 2 * way, j - 1)

    def fill_beyond(way):
        for away in (1, 2):
            target = lax.rem(place + (away if way == 0 else ring - away), ring)
            fill_slots(way * far + relay - 1, 2 * far + away + 2 * way, target)

    def pick(way, j):
        table, pair = beyond(way, j)
        parts = []
        for k in range(CAP):
            block = jnp.maximum(blk_s[table * slots + pair * CAP + k], 0)
            held = qlast[way][block // (CHUNK // BLOCK)].astype(jnp.float32)
            turned = pltpu.roll(held, BLOCK, 1)
            parts.append(jnp.where(block % (CHUNK // BLOCK) == k, held, turned))
        picked[way, j] = jnp.where(lanes < BLOCK, parts[0], parts[1]).astype(jnp.bfloat16)

    def project(j):
        total = jnp.zeros((CHUNK, HEAD_DIM), jnp.float32)
        logits = jnp.zeros((wg.shape[0], CHUNK), jnp.float32)
        for r in range(4):
            features = pl.ds(pl.multiple_of(x_source[r] * width, width), width)
            part = tbuf[j, r]
            total = total + jnp.dot(part, wq[features], preferred_element_type=jnp.float32)
        qown[j] = total.T.astype(jnp.bfloat16)
        for r in range(4):
            features = pl.ds(pl.multiple_of(x_source[r] * width, width), width)
            logits = logits + lax.dot_general(
                wg[:, features], tbuf[j, r], (((1,), (1,)), ((), ())), preferred_element_type=jnp.float32
            )
        heads = lax.broadcasted_iota(jnp.int32, logits.shape, 0)
        logit = jnp.sum(jnp.where(heads == head, logits, 0.0), 0, keepdims=True)
        gate[j] = jax.nn.sigmoid(logit)

    def make_keys(part):
        count = passages // KV_PARTS
        part_rows = store[pl.ds(part * count * rows, count * rows)]
        made = jnp.dot(part_rows, wk[...], preferred_element_type=jnp.float32).astype(jnp.bfloat16)
        for i in range(count):
            kall[core, part * count + i] = made[i * rows : (i + 1) * rows]

    def make_values(part):
        count = passages // KV_PARTS
        part_rows = store[pl.ds(part * count * rows, count * rows)]
        made = jnp.dot(part_rows, wv[...], preferred_element_type=jnp.float32)
        for i in range(count):
            vall[core, part * count + i] = made[i * rows : (i + 1) * rows].T.astype(jnp.bfloat16)

    def retention(sequence):
        span = pl.ds(sequence * SEQ_LEN, SEQ_LEN)
        halfway = RET_DIM // 2

        def turned(values, scale):
            leading = values[:, :halfway].astype(jnp.float32)
            trailing = values[:, halfway:].astype(jnp.float32)
            c, s = cosines[...], sines[...]
            both = jnp.concatenate([leading * c - trailing * s, leading * s + trailing * c], 1)
            return (both * scale if scale != 1.0 else both).astype(jnp.bfloat16)

        log_gamma = jnp.float32(0.0)
        for h in range(xs):
            log_gamma = jnp.where(head == h, jnp.float32(math.log1p(-(2.0 ** (-5 - h)))), log_gamma)
        grid = (SEQ_LEN, SEQ_LEN)
        offsets = lax.broadcasted_iota(jnp.int32, grid, 0) - lax.broadcasted_iota(jnp.int32, grid, 1)
        distance = jnp.maximum(offsets, 0).astype(jnp.float32)
        decays = jnp.where(offsets >= 0, jnp.exp(log_gamma * distance), 0.0)
        scores = lax.dot_general(
            turned(rq[span], 1.0), turned(rk[span], RET_DIM ** (-0.5)),
            (((1,), (1,)), ((), ())), preferred_element_type=jnp.float32,
        )
        raw = jnp.dot((scores * decays).astype(jnp.bfloat16), rv[span], preferred_element_type=jnp.float32)
        centred = raw - jnp.mean(raw, -1, keepdims=True)
        normed = centred * lax.rsqrt(jnp.mean(centred * centred, -1, keepdims=True) + NORM_EPS)
        out_ref[span, 0:RET_DIM] = normed.astype(jnp.bfloat16)

    def merge(first, first_ml, second, second_ml):
        top = jnp.maximum(first_ml[0], second_ml[0])
        left_scale, right_scale = jnp.exp(first_ml[0] - top), jnp.exp(second_ml[0] - top)
        summed = first * left_scale + second * right_scale
        total = first_ml[1] * left_scale + second_ml[1] * right_scale
        return summed, (top, total)

    for piece in range(3):
        for way in ways:
            x_copy(way, 1, piece).start()
    ids_flat[...] = jnp.zeros_like(ids_flat)
    ids_flat[:, :block_count] = ids_ref[...]
    padded = ids_flat[...]
    row = padded[0:1]
    for slot in range(1, NPB):
        row = row + pltpu.roll(padded[slot : slot + 1], slot * block_count, 1)
    ids_row[...] = row

    def x_forward(piece):
        for way in ways:
            x_copy(way, 1, piece).wait_recv()
            x_copy(way, 2, piece).start()
            if 1 <= piece < pieces - 2:
                x_copy(way, 1, piece + 2).start()

    def q_make(j):
        token_loads[j].wait()
        for piece in range(j * (CHUNK // PIECE), (j + 1) * (CHUNK // PIECE)):
            for way in ways:
                x_copy(way, 2, piece).wait_recv()
        project(j)

    def q_send_first(j):
        for way in ways:
            q_copy(way, 1, j).start()

    def arrive(hop, j, forward=True):
        for way in ways:
            q_copy(way, hop, j).wait_recv()
            if forward:
                q_copy(way, hop + 1, j).start()

    def m_arrive(hop, forward):
        for way in ways:
            m_copy(way, hop).wait_recv()
            if forward:
                m_copy(way, hop + 1).start()
            fetch_ids(ids_in.at[way, hop - 1], way * far + hop - 1).start()

    def m_fill(hop):
        for way in ways:
            fetch_ids(ids_in.at[way, hop - 1], way * far + hop - 1).wait()
            fill_slots(way * far + hop - 1, way * far + hop - 1, place)

    x_forward(0)
    for way in ways:
        m_copy(way, 1).start()
    fetch_ids(ids_row, 2 * far).start()
    loads[0].wait()
    loads[1].wait()
    make_keys(0)
    x_forward(1)
    make_keys(1)
    x_forward(2)
    make_keys(2)
    loads[3].wait()
    loads[4].wait()
    q_make(0)
    q_send_first(0)
    loads[2].wait()
    kv_copy(0).start()
    x_forward(3)
    make_values(0)
    make_values(1)
    x_forward(4)
    q_make(1)
    q_send_first(1)
    x_forward(5)
    make_values(2)
    fetch_ids(ids_row, 2 * far).wait()
    fill_slots(2 * far, 2 * far, place)
    for copy in loads[5:]:
        copy.start()
    m_arrive(1, True)
    arrive(1, 0)
    kv_copy(1).start()
    x_forward(6)
    q_make(2)
    m_fill(1)
    q_send_first(2)
    arrive(1, 1)
    x_forward(7)
    q_make(3)
    for i in range(2):
        kv_copy(i).wait()
    q_send_first(3)

    def attend_own(first):
        @pl.loop(first, first + 2)
        def _(j):
            weighted, highest, total = attend(qown[j], 2 * far, j)
            loc0[j] = weighted.astype(jnp.bfloat16)
            loc0ml[j, 0:1] = highest
            loc0ml[j, 1:2] = total

    def attend_both(hop, j):
        attend_hop(hop, [(way, j) for way in ways])

    def pass_hop(hop):
        m_arrive(hop, True)

        @pl.loop(0, chunks)
        def _(j):
            arrive(hop, j)
            attend_both(hop - 1, j)

        m_fill(hop)

    attend_own(0)
    arrive(1, 2)
    attend_own(2)
    m_arrive(2, True)

    @pl.loop(0, 2)
    def _(j):
        arrive(2, j, relay > 2)
        attend_both(1, j)

    arrive(1, 3)

    @pl.loop(2, chunks)
    def _(j):
        attend_both(1, j)
        arrive(2, j, relay > 2)

    m_fill(2)
    if relay > 3:

        @pl.loop(3, relay - 1)
        def _(hop):
            pass_hop(hop)

        pass_hop(relay - 1)
    if relay > 2:
        m_arrive(relay, True)
        m_fill(relay)
    for way in ways:
        fill_beyond(way)
    if relay > 2:

        @pl.loop(0, chunks - 1)
        def _(j):
            arrive(relay, j, False)
            attend_both(relay - 1, j)

        arrive(relay, chunks - 1, False)
    for j in range(2):
        for way in ways:
            pick(way, j)
        for way in ways:
            q_copy(way, relay + 1, j).start()
    for way in ways:
        pick(way, 2)
    if relay > 2:
        attend_both(relay - 1, chunks - 1)
    for way in ways:
        q_copy(way, relay + 1, 0).wait_recv()
        q_copy(way, far, 0).start()
    for way in ways:
        q_copy(way, relay + 1, 2).start()

    def r_start(way, hop, j):
        for copy in r_copies(way, hop, j):
            copy.start()

    def r_merge(way, hop, j):
        for copy in r_copies(way, hop + 1, j):
            copy.wait_recv()
        summed, (top, total) = merge(
            rbuf[way, hop, j].astype(jnp.float32),
            (rml[way, hop, j, 0:1], rml[way, hop, j, 1:2]),
            loc[1 - way, hop - 1, j].astype(jnp.float32),
            (locml[1 - way, hop - 1, j, 0:1], locml[1 - way, hop - 1, j, 1:2]),
        )
        loc[1 - way, hop - 1, j] = summed.astype(jnp.bfloat16)
        locml[1 - way, hop - 1, j, 0:1] = top
        locml[1 - way, hop - 1, j, 1:2] = total

    def r_scatter(way, j):
        data = [loc[1 - way, relay - 1, j].astype(jnp.float32)]
        tops = [locml[1 - way, relay - 1, j, 0:1]]
        totals = [locml[1 - way, relay - 1, j, 1:2]]
        valid = [None]
        for message in range(3):
            table, pair = beyond(1 - way, message)
            came = rbuf[way, relay, message].astype(jnp.float32)
            came_top, came_total = rml[way, relay, message, 0:1], rml[way, relay, message, 1:2]
            blocks = [blk_s[table * slots + pair * CAP + k] for k in range(CAP)]
            for shift in range(CAP):
                first, second = blocks[shift], blocks[1 - shift]
                wanted = jnp.where(lanes < BLOCK, first - j * CAP, second - j * CAP - 1) == 0
                if shift:
                    came, came_top, came_total = (
                        pltpu.roll(came, BLOCK, 1),
                        pltpu.roll(came_top, BLOCK, 1),
                        pltpu.roll(came_total, BLOCK, 1),
                    )
                data.append(came)
                tops.append(jnp.where(wanted, came_top, FLOOR))
                totals.append(came_total)
                valid.append(wanted)
        top = tops[0]
        for other in tops[1:]:
            top = jnp.maximum(top, other)
        summed, total = None, None
        for value, own_top, own_total, wanted in zip(data, tops, totals, valid):
            scale = jnp.exp(own_top - top)
            if wanted is None:
                summed, total = value * scale, own_total * scale
            else:
                scale = jnp.where(wanted, scale, 0.0)
                summed, total = summed + value * scale, total + own_total * scale
        loc[1 - way, relay - 1, j] = summed.astype(jnp.bfloat16)
        locml[1 - way, relay - 1, j, 0:1] = top
        locml[1 - way, relay - 1, j, 1:2] = total

    m_arrive(far - 1, True)

    @pl.loop(0, 2)
    def _(j):
        attend_both(relay, j)

    m_fill(far - 1)
    for way in ways:
        q_copy(way, far - 1, 1).wait_recv()
    for way in ways:
        attend_pair(far - 1, way, 1, 0)
    m_arrive(far, False)
    m_fill(far)
    for way in ways:
        q_copy(way, far, 0).wait_recv()
    for way in ways:
        attend_pair(far, way, 0, way)
    for way in ways:
        r_start(way, far, 0)
    for way in ways:
        r_start(way, far - 1, 1)
    for way in ways:
        q_copy(way, far - 1, 2).wait_recv()
    for way in ways:
        attend_pair(far - 1, way, 2, 1)
    for way in ways:
        for copy in r_copies(way, far, 0):
            copy.wait_recv()
        r_start(way, far - 1, 0)
    for way in ways:
        r_start(way, far - 1, 2)

    @pl.loop(2, chunks)
    def _(j):
        attend_both(relay, j)

    for copy in loads[5:]:
        copy.wait()
    retention(0)
    retention(1)

    for message in (1, 0, 2):
        for way in ways:
            for copy in r_copies(way, far - 1, message):
                copy.wait_recv()
    for j in range(chunks):
        for way in ways:
            r_scatter(way, j)
        for way in ways:
            r_start(way, relay, j)

    @pl.loop(1, relay)
    def _(step):
        hop = relay - step
        for j in range(chunks):
            for way in ways:
                r_merge(way, hop, j)
            for way in ways:
                r_start(way, hop, j)

    def finish(j):
        summed, both = loc0[j].astype(jnp.float32), (loc0ml[j, 0:1], loc0ml[j, 1:2])
        for way in ways:
            summed, both = merge(
                summed, both, rbuf[way, 0, j].astype(jnp.float32), (rml[way, 0, j, 0:1], rml[way, 0, j, 1:2])
            )
        share = (summed * (gate[j] / both[1])).T
        out_ref[j * CHUNK : (j + 1) * CHUNK, RET_DIM:] = share.astype(jnp.bfloat16)

    for j in range(chunks):
        for way in ways:
            for copy in r_copies(way, 1, j):
                copy.wait_recv()
        finish(j)

    for j in range(chunks):
        for way in ways:
            q_copy(way, 1, j).wait_send()
    for way in ways:
        m_copy(way, 1).wait_send()
        for piece in range(pieces):
            for hop in (1, 2):
                x_copy(way, hop, piece).wait_send()

    @pl.loop(2, far + 1)
    def _(hop):
        for way in ways:
            m_copy(way, hop).wait_send()

    @pl.loop(2, relay)
    def _(hop):
        for j in range(chunks):
            for way in ways:
                q_copy(way, hop, j).wait_send()

    @pl.loop(1, relay + 1)
    def _(hop):
        for j in range(chunks):
            for way in ways:
                for copy in r_copies(way, hop, j):
                    copy.wait_send()

    for way in ways:
        for j in range(chunks):
            q_copy(way, relay, j).wait_send()
        for hop, count in ((far - 1, 3), (far, 1)):
            for j in range(count):
                q_copy(way, hop, j).wait_send()
                for copy in r_copies(way, hop, j):
                    copy.wait_send()


def body(
    tokens, ret_query, ret_key, ret_value, w_query, w_key, w_value, w_gate, store, passage_ids
):
    ring = lax.axis_size("st") // CORES
    far = ring // 2
    xs = lax.axis_size("tp")
    token_count, width = tokens.shape
    chunks = token_count // CHUNK
    passages, rows, features = store.shape
    slots = CAP * CORES
    assert xs == 4 and far >= 4 and chunks == 4 and CHUNK == CAP * BLOCK and w_query.shape[1] == HEAD_DIM and passages % KV_PARTS == 0
    assert passage_ids.size <= 128
    cosines, sines = rotary_tables()
    buffer = (2, far, chunks, HEAD_DIM, CHUNK)
    stats = (2, far, chunks, 2, CHUNK)
    flags = (2, far, chunks)
    dma = pltpu.SemaphoreType.DMA
    bf16, f32, i32 = jnp.bfloat16, jnp.float32, jnp.int32
    hbm = pl.BlockSpec(memory_space=pl.ANY)
    vmem = pl.BlockSpec(memory_space=pltpu.VMEM)
    return pl.pallas_call(
        mixer_kernel,
        out_shape=jax.ShapeDtypeStruct((token_count, RET_DIM + HEAD_DIM), bf16),
        in_specs=[vmem] + [hbm] * 11,
        out_specs=vmem,
        scratch_shapes=[
            pltpu.VMEM((chunks, 4, CHUNK, width), bf16),
            pltpu.VMEM(w_query.shape, bf16),
            pltpu.VMEM(w_key.shape, bf16),
            pltpu.VMEM(w_value.shape, bf16),
            pltpu.VMEM(w_gate.shape[::-1], bf16),
            pltpu.VMEM((passages * rows, features), bf16),
            pltpu.VMEM(ret_query.shape, bf16),
            pltpu.VMEM(ret_query.shape, bf16),
            pltpu.VMEM(ret_query.shape, bf16),
            pltpu.VMEM(cosines.shape, f32),
            pltpu.VMEM(sines.shape, f32),
            pltpu.SMEM((2 * far + 1, 1, 128), i32),
            pltpu.SMEM(((2 * far + 5) * slots,), i32),
            pltpu.SMEM(((2 * far + 5) * slots,), i32),
            pltpu.VMEM((NPB, 128), i32),
            pltpu.VMEM((1, 128), i32),
            pltpu.VMEM((2, far, 1, 128), i32),
            pltpu.VMEM(buffer[2:], bf16),
            pltpu.VMEM((chunks, 1, CHUNK), f32),
            pltpu.VMEM(buffer, bf16),
            pltpu.VMEM(buffer[2:], bf16),
            pltpu.VMEM(buffer[2:], bf16),
            pltpu.VMEM((2, 3) + buffer[3:], bf16),
            pltpu.VMEM((CORES, passages, rows, HEAD_DIM), bf16),
            pltpu.VMEM((CORES, passages, HEAD_DIM, rows), bf16),
            pltpu.VMEM(buffer, bf16),
            pltpu.VMEM(stats, f32),
            pltpu.VMEM(buffer[2:], bf16),
            pltpu.VMEM(stats[2:], f32),
            pltpu.VMEM(buffer, bf16),
            pltpu.VMEM(stats, f32),
            dma((10,)),
            dma((2 * far + 1,)),
            dma((chunks,)),
            dma((2,)),
            dma((2,)),
            dma((2, 2, token_count // PIECE)),
            dma((2, 2, token_count // PIECE)),
            dma((2, far)),
            dma((2, far)),
            dma(flags),
            dma(flags),
            dma(flags),
            dma(flags),
            dma(flags),
            dma(flags),
        ],
        compiler_params=pltpu.CompilerParams(
            collective_id=0, has_side_effects=True, vmem_limit_bytes=60 * 1024 * 1024
        ),
    )(
        passage_ids.T, tokens, ret_query, ret_key, ret_value, w_query, w_key, w_value, w_gate.T,
        store.reshape(passages * rows, features), jnp.asarray(cosines), jnp.asarray(sines),
    )


def solution(mesh):
    placed = (
        P(("grp", "st"), "tp"),
        P(("grp", "st"), "tp"),
        P(("grp", "st"), "tp"),
        P(("grp", "st"), "tp"),
        P(None, "tp"),
        P(None, "tp"),
        P(None, "tp"),
        P(),
        P("st", None, None),
        P(("grp", "st"), None),
    )
    return jax.shard_map(
        body, mesh=mesh, in_specs=placed, out_specs=P(("grp", "st"), "tp"), check_vma=False
    )
```
